32 devices in a mesh: grp: 2 (over y), sp: 4 (over z), tp: 4 (over x, core).
Axes of the slice: x: 2, y: 2, z: 4, core: 2. Of those that a mesh axis runs over, the one named last changes fastest.
Arguments:
- resid_in: bfloat16 [2048, 2048], P(('grp', 'sp', 'tp')), parts along dimension 0, may hold values from -3 to 3
- queries: bfloat16 [2048, 1024], P(('grp', 'sp'), 'tp'), parts along dimension 0, may hold values from -39 to 39
- keys: bfloat16 [2048, 1024], P(('grp', 'sp'), 'tp'), parts along dimension 0, may hold values from -6 to 6
- values: bfloat16 [2048, 1024], P(('grp', 'sp'), 'tp'), parts along dimension 0, may hold values from -12 to 12
- cum_gate: float32 [2048, 16], P('grp', 'tp'), parts along dimension 0, may hold values from -105 to 0, as said below
- w_out: bfloat16 [1024, 2048], replicated, may hold values from -0.1875 to 0.1875
- norm_gain: float32 [2048], replicated, may hold values from 0.1 to 1.9
- w_gate: bfloat16 [2048, 5632], P('sp', 'tp'), may hold values from -0.125 to 0.125
- w_up: bfloat16 [2048, 5632], P('sp', 'tp'), may hold values from -0.125 to 0.125
- w_down: bfloat16 [5632, 2048], P('tp', 'sp'), may hold values from -0.078125 to 0.078125
Outputs:
- resid_out: bfloat16 [2048, 2048], P(('grp', 'sp', 'tp')), parts along dimension 0
The draws below stay inside these ranges and needn't reach their ends.
There are 2 independent parts, one for each index of `grp`. The reference program is written for one: setup_inputs(seed, part) draws one part's arguments, and reference() takes and returns one part's arrays. A program takes and returns all parts, laid end to end along the dimension named above; an argument that names none is the same for every part. Nothing has to cross between parts.
Inputs may be any that keep to these rules, and one draw needn't show every extreme that they name: `cum_gate`: in every head the values never rise from one position to the next, and the first is at most 0.
All inputs are finite; a program needn't handle non-finite values.
Results may differ from the reference program's by a relative error of at most 0.018.
Values may be sent and summed in bfloat16 or wider, within the bound.
A program may use at most 128 MiB of HBM per device.

```python
import math
import jax
import jax.numpy as jnp
from jax import lax

D = 2048
HEADS = 16
HEAD_DIM = 64
FF = 5632
TOK_DEV = 256
SEQUENCE_TOKENS = 1024
ATT_WIDTH = 1024


def attention_pair(key):
    key_q, key_k = jax.random.split(key, 2)
    width = HEADS * HEAD_DIM
    queries = 2.0 * jnp.clip(jax.random.normal(key_q, (SEQUENCE_TOKENS, width), jnp.float32), -6.0, 6.0)
    keys = jnp.clip(jax.random.normal(key_k, (SEQUENCE_TOKENS, width), jnp.float32), -6.0, 6.0)
    return (queries, keys)


def draw_queries(key, part):
    return attention_pair(jax.random.fold_in(key, 11))[0].astype(jnp.bfloat16)


def draw_keys(key, part):
    return attention_pair(jax.random.fold_in(key, 11))[1].astype(jnp.bfloat16)


def draw_cum_gate(key, part):
    every_key_row = jax.random.split(jax.random.fold_in(key, 23), 6)
    sluggish_path = jax.random.permutation(every_key_row[0], HEADS) < HEADS // 2
    fast_rate = jnp.exp(jax.random.uniform(every_key_row[1], (HEADS,), jnp.float32, jnp.log(1.0 / 100.0), jnp.log(1.0 / 30.0)))
    rate = jnp.where(sluggish_path, 0.4 / SEQUENCE_TOKENS, fast_rate)
    factor = jnp.exp(jax.random.uniform(every_key_row[2], (SEQUENCE_TOKENS // TOK_DEV, 1), jnp.float32, jnp.log(0.5), jnp.log(2.0)))
    factor = jnp.repeat(factor, TOK_DEV, axis=0)
    rough = jax.random.uniform(every_key_row[3], (SEQUENCE_TOKENS, HEADS), jnp.float32, 0.5, 1.5)
    step_count = -rate[None, :] * factor * rough
    spike_position = jax.random.randint(every_key_row[4], (3,), 1, SEQUENCE_TOKENS, dtype=jnp.int32)
    training_loss = jax.random.uniform(every_key_row[5], (3, HEADS), jnp.float32, 0.2, 0.5)
    step_count = step_count.at[spike_position].add(jnp.log(1.0 - training_loss) * sluggish_path.astype(jnp.float32)[None, :])
    return jnp.cumsum(step_count, axis=0)


def levels(key, shape, cuts, low, top_value):
    factor_of, own = 1.0, jax.random.fold_in(key, 6)
    for position, shards_of in cuts:
        draws = jnp.exp(jax.random.uniform(jax.random.fold_in(own, position), (shards_of,), jnp.float32, low / len(cuts), top_value / len(cuts)))
        factor_of = factor_of * jnp.repeat(draws, shape[position] // shards_of).reshape([-1 if axis == position else 1 for axis in range(len(shape))])
    return factor_of


def scatter_about(key, shape, spread, reach, pieces=(), held_as=jnp.bfloat16):
    gain = levels(key, shape, pieces, -0.22, 0.18) if pieces else 1.0
    drawn = jax.random.normal(key, shape, jnp.float32) * spread * gain
    return jnp.minimum(jnp.maximum(drawn, -reach), reach).astype(held_as)


def setup_inputs(seed: int = 0, part: int = 0) -> dict:
    splits = jax.random.split(jax.random.key(seed), 11)
    part_splits = jax.random.split(jax.random.fold_in(splits[10], part), 11)
    return {
        "resid_in": scatter_about(part_splits[0], (SEQUENCE_TOKENS, D), 0.5, 3.0, ((0, 16),)),
        "queries": draw_queries(jax.random.fold_in(jax.random.fold_in(splits[10], part), 71), part),
        "keys": draw_keys(jax.random.fold_in(jax.random.fold_in(splits[10], part), 71), part),
        "values": scatter_about(part_splits[3], (SEQUENCE_TOKENS, ATT_WIDTH), 2.0, 12.0, ((0, 4), (1, 4))),
        "cum_gate": draw_cum_gate(jax.random.fold_in(jax.random.fold_in(splits[10], part), 71), part),
        "w_out": scatter_about(splits[5], (ATT_WIDTH, D), ATT_WIDTH ** -0.5, 0.1875),
        "norm_gain": jnp.clip(1.0 + 0.18 * jax.random.normal(splits[6], (D,), jnp.float32), 0.1, 1.9),
        "w_gate": scatter_about(splits[7], (D, FF), D ** -0.5, 0.125, ((0, 4), (1, 4))),
        "w_up": scatter_about(splits[8], (D, FF), D ** -0.5, 0.125, ((0, 4), (1, 4))),
        "w_down": scatter_about(splits[9], (FF, D), FF ** -0.5, 0.078125, ((0, 4), (1, 4))),
    }


def attention(queries, keys, values, cum_gate):
    total = queries.shape[0]
    span = math.gcd(total, 256)
    scale = HEAD_DIM ** (-0.5)
    query_heads = queries.astype(jnp.float32).reshape(total, HEADS, HEAD_DIM)
    key_heads = keys.astype(jnp.float32).reshape(total, HEADS, HEAD_DIM)
    value_heads = values.astype(jnp.float32).reshape(total, HEADS, HEAD_DIM)
    positions = jnp.arange(total, dtype=jnp.int32)

    def block(first):
        query_block = lax.dynamic_slice_in_dim(query_heads, first, span, 0)
        gate_block_rows = lax.dynamic_slice_in_dim(cum_gate, first, span, 0)
        scores = jnp.einsum('qhd,khd->hqk', query_block, key_heads) * scale
        scores = scores + gate_block_rows.T[:, :, None] - cum_gate.T[:, None, :]
        mask = positions[None, :] <= (first + jnp.arange(span, dtype=jnp.int32))[:, None]
        scores = jnp.where(mask[None], scores, -1e+30)
        top = lax.optimization_barrier(jnp.max(scores, axis=-1, keepdims=True))
        weights = jnp.where(mask[None], jnp.exp(scores - top), 0.0)
        totals = lax.optimization_barrier(jnp.sum(weights, axis=-1))
        rounded = lax.optimization_barrier(weights.astype(jnp.bfloat16)).astype(jnp.float32)
        attended = jnp.einsum('hqk,khd->qhd', rounded, value_heads) / totals.T[:, :, None]
        return attended.reshape(span, HEADS * HEAD_DIM).astype(jnp.bfloat16)
    starts = jnp.arange(total // span, dtype=jnp.int32) * span
    return lax.map(block, starts).reshape(total, HEADS * HEAD_DIM)

def reference(resid_in, queries, keys, values, cum_gate, w_out, norm_gain, w_gate, w_up, w_down):
    attended = attention(queries, keys, values, cum_gate)
    mixed = jnp.dot(attended, w_out, preferred_element_type=jnp.float32)
    resid = resid_in.astype(jnp.float32) + mixed
    normed = resid * lax.rsqrt(lax.optimization_barrier(jnp.mean(resid * resid, axis=-1, keepdims=True)) + 1e-06)
    normed = (normed * norm_gain).astype(jnp.bfloat16)
    gate = jnp.dot(normed, w_gate, preferred_element_type=jnp.float32)
    up = jnp.dot(normed, w_up, preferred_element_type=jnp.float32)
    hidden = (jax.nn.silu(gate) * up).astype(jnp.bfloat16)
    down = jnp.dot(hidden, w_down, preferred_element_type=jnp.float32)
    return (resid + down).astype(jnp.bfloat16)
```

```python
import math

import jax
import jax.numpy as jnp
from jax import lax
from jax.sharding import PartitionSpec as P

HEAD_DIM = 64


def on_device(resid_in, queries, keys, values, cum_gate, w_out, norm_gain, w_gate, w_up, w_down):
    tok_rows = queries.shape[0]
    local_heads = queries.shape[1] // HEAD_DIM
    scale = HEAD_DIM ** (-0.5)
    offset = lax.axis_index("sp") * tok_rows
    query_heads = queries.reshape(tok_rows, local_heads, HEAD_DIM)
    own_gate = lax.dynamic_slice_in_dim(cum_gate, offset, tok_rows, 0).T
    query_pos = offset + jnp.arange(tok_rows, dtype=jnp.int32)
    last_pos = offset + tok_rows - 1
    initial = (
        jnp.full((local_heads, tok_rows), -1e30, jnp.float32),
        jnp.zeros((local_heads, tok_rows), jnp.float32),
        jnp.zeros((tok_rows, local_heads, HEAD_DIM), jnp.float32),
    )
    pair = lax.all_gather(jnp.stack([keys, values]), "sp", axis=1, tiled=True)
    key_piece, value_piece = pair[0], pair[1]
    length = key_piece.shape[0]
    span = math.gcd(length, 512)

    def block(index, state):
        begin = index * span

        def work(inner):
            maxima, totals, summed = inner
            key_block = lax.dynamic_slice_in_dim(key_piece, index * span, span, 0).reshape(
                span, local_heads, HEAD_DIM
            )
            value_block_rows = lax.dynamic_slice_in_dim(value_piece, index * span, span, 0).reshape(
                span, local_heads, HEAD_DIM
            )
            key_gate = lax.dynamic_slice_in_dim(cum_gate, begin, span, 0).T
            scores = (
                jnp.einsum(
                    "qhd,khd->hqk", query_heads, key_block, preferred_element_type=jnp.float32
                )
                * scale
            )
            scores = scores + own_gate[:, :, None] - key_gate[:, None, :]
            key_pos = begin + jnp.arange(span, dtype=jnp.int32)
            mask = (key_pos[None, :] <= query_pos[:, None])[None]
            scores = jnp.where(mask, scores, -1e30)
            new_max = jnp.maximum(maxima, jnp.max(scores, axis=-1))
            weights = jnp.where(mask, jnp.exp(scores - new_max[:, :, None]), 0.0)
            rescale = jnp.exp(maxima - new_max)
            totals = totals * rescale + jnp.sum(weights, axis=-1)
            product = jnp.einsum(
                "hqk,khd->qhd",
                weights.astype(jnp.bfloat16),
                value_block_rows,
                preferred_element_type=jnp.float32,
            )
            summed = summed * rescale.T[:, :, None] + product
            return (new_max, totals, summed)

        return lax.cond(begin <= last_pos, work, lambda inner: inner, state)

    maxima, totals, summed = lax.fori_loop(0, length // span, block, initial)
    attended = (
        (summed / totals.T[:, :, None])
        .reshape(tok_rows, local_heads * HEAD_DIM)
        .astype(jnp.bfloat16)
    )
    head_rows = lax.all_to_all(attended, "tp", split_axis=0, concat_axis=1, tiled=True)
    mixed = jnp.dot(head_rows, w_out, preferred_element_type=jnp.float32)
    resid = resid_in.astype(jnp.float32) + mixed
    normed = resid * lax.rsqrt(jnp.mean(resid * resid, axis=-1, keepdims=True) + 1e-06)
    normed = (normed * norm_gain).astype(jnp.bfloat16)
    all_rows = lax.all_gather(normed, ("sp", "tp"), axis=0, tiled=True)
    full_gate, full_up, full_down = (
        lax.all_to_all(w_gate, "sp", split_axis=1, concat_axis=0, tiled=True),
        lax.all_to_all(w_up, "sp", split_axis=1, concat_axis=0, tiled=True),
        lax.all_to_all(w_down, "sp", split_axis=0, concat_axis=1, tiled=True),
    )
    gate = jnp.dot(all_rows, full_gate, preferred_element_type=jnp.float32)
    up = jnp.dot(all_rows, full_up, preferred_element_type=jnp.float32)
    hidden = (jax.nn.silu(gate) * up).astype(jnp.bfloat16)
    terms = jnp.dot(hidden, full_down, preferred_element_type=jnp.float32)
    back = lax.psum_scatter(
        terms.astype(jnp.bfloat16), ("sp", "tp"), scatter_dimension=0, tiled=True
    ).astype(jnp.float32)
    return (resid + back).astype(jnp.bfloat16)


def solution(mesh):
    return jax.shard_map(
        on_device,
        mesh=mesh,
        in_specs=(
            P(("grp", "sp", "tp"), None),
            P(("grp", "sp"), "tp"),
            P(("grp", "sp"), "tp"),
            P(("grp", "sp"), "tp"),
            P("grp", "tp"),
            P(),
            P(),
            P("sp", "tp"),
            P("sp", "tp"),
            P("tp", "sp"),
        ),
        out_specs=P(("grp", "sp", "tp"), None),
        check_vma=False,
    )
```

```python
import functools
import math

import jax
import jax.numpy as jnp
from jax import lax
from jax.experimental import pallas as pl
from jax.experimental.pallas import tpu as pltpu
from jax.sharding import PartitionSpec as P

HEAD_DIM = 64


def on_device(resid_in, queries, keys, values, cum_gate, w_out, norm_gain, w_gate, w_up, w_down):
    tok_rows = queries.shape[0]
    local_heads = queries.shape[1] // HEAD_DIM
    scale = HEAD_DIM ** (-0.5)
    offset = lax.axis_index("sp") * tok_rows
    query_heads = queries.reshape(tok_rows, local_heads, HEAD_DIM)
    own_gate = lax.dynamic_slice_in_dim(cum_gate, offset, tok_rows, 0).T
    query_pos = offset + jnp.arange(tok_rows, dtype=jnp.int32)
    last_pos = offset + tok_rows - 1
    initial = (
        jnp.full((local_heads, tok_rows), -1e30, jnp.float32),
        jnp.zeros((local_heads, tok_rows), jnp.float32),
        jnp.zeros((tok_rows, local_heads, HEAD_DIM), jnp.float32),
    )
    pair = lax.all_gather(jnp.stack([keys, values]), "sp", axis=1, tiled=True)
    key_piece, value_piece = pair[0], pair[1]
    length = key_piece.shape[0]
    span = math.gcd(length, 512)

    def block(index, state):
        begin = index * span

        def work(inner):
            maxima, totals, summed = inner
            key_block = lax.dynamic_slice_in_dim(key_piece, index * span, span, 0).reshape(
                span, local_heads, HEAD_DIM
            )
            value_block_rows = lax.dynamic_slice_in_dim(value_piece, index * span, span, 0).reshape(
                span, local_heads, HEAD_DIM
            )
            key_gate = lax.dynamic_slice_in_dim(cum_gate, begin, span, 0).T
            scores = (
                jnp.einsum(
                    "qhd,khd->hqk", query_heads, key_block, preferred_element_type=jnp.float32
                )
                * scale
            )
            scores = scores + own_gate[:, :, None] - key_gate[:, None, :]
            key_pos = begin + jnp.arange(span, dtype=jnp.int32)
            mask = (key_pos[None, :] <= query_pos[:, None])[None]
            scores = jnp.where(mask, scores, -1e30)
            new_max = jnp.maximum(maxima, jnp.max(scores, axis=-1))
            weights = jnp.where(mask, jnp.exp(scores - new_max[:, :, None]), 0.0)
            rescale = jnp.exp(maxima - new_max)
            totals = totals * rescale + jnp.sum(weights, axis=-1)
            product = jnp.einsum(
                "hqk,khd->qhd",
                weights.astype(jnp.bfloat16),
                value_block_rows,
                preferred_element_type=jnp.float32,
            )
            summed = summed * rescale.T[:, :, None] + product
            return (new_max, totals, summed)

        return lax.cond(begin <= last_pos, work, lambda inner: inner, state)

    maxima, totals, summed = lax.fori_loop(0, length // span, block, initial)
    attended = (
        (summed / totals.T[:, :, None])
        .reshape(tok_rows, local_heads * HEAD_DIM)
        .astype(jnp.bfloat16)
    )
    head_rows = lax.all_to_all(attended, "tp", split_axis=0, concat_axis=1, tiled=True)
    mixed = jnp.dot(head_rows, w_out, preferred_element_type=jnp.float32)
    resid = resid_in.astype(jnp.float32) + mixed
    normed = resid * lax.rsqrt(jnp.mean(resid * resid, axis=-1, keepdims=True) + 1e-06)
    normed = (normed * norm_gain).astype(jnp.bfloat16)
    all_rows = lax.all_gather(normed, ("sp", "tp"), axis=0, tiled=True)
    full_gate, full_up, full_down = (
        lax.all_to_all(w_gate, "sp", split_axis=1, concat_axis=0, tiled=True),
        lax.all_to_all(w_up, "sp", split_axis=1, concat_axis=0, tiled=True),
        lax.all_to_all(w_down, "sp", split_axis=0, concat_axis=1, tiled=True),
    )
    gate = jnp.dot(all_rows, full_gate, preferred_element_type=jnp.float32)
    up = jnp.dot(all_rows, full_up, preferred_element_type=jnp.float32)
    hidden = (jax.nn.silu(gate) * up).astype(jnp.bfloat16)
    terms = jnp.dot(hidden, full_down, preferred_element_type=jnp.float32)
    back = lax.psum_scatter(
        terms.astype(jnp.bfloat16), ("sp", "tp"), scatter_dimension=0, tiled=True
    ).astype(jnp.float32)
    return (resid + back).astype(jnp.bfloat16)


MESH = pl.DeviceIdType.MESH
F32 = jnp.float32
BF16 = jnp.bfloat16


def layer_kernel(
    dims, resid_ref, q_ref, k_ref, v_ref, gate_ref, gate_t_ref, gain_ref, w_out_ref, w_gate_ref,
    w_up_ref, w_down_ref, out_ref, kbuf, vbuf, top, tot, acc, att, heads, w_out, resid, nall, wg,
    wu, wd, part, crecv, csend, keep, xrecv, zsend, zrecv, loc_sem, kv_send, kv_recv, wz_send,
    wz_recv, wy_send, wy_recv, h_send, h_recv, az_send, az_recv, ax_send, ax_recv, ac_send,
    ac_recv, rc_send, rc_recv, rx_send, rx_recv, rz_send, rz_recv,
):
    ns, nt, chunk = dims
    g, s, t = lax.axis_index("grp"), lax.axis_index("sp"), lax.axis_index("tp")
    rows, width = resid_ref.shape
    tok, att_w = q_ref.shape
    depth, units = w_gate_ref.shape
    nheads = att_w // HEAD_DIM
    half_depth, half_chunk = depth // 2, chunk // 2
    x, c = t // 2, t % 2
    tx = (t + 2) % 4
    tc = t + 1 - 2 * c
    scale = HEAD_DIM ** (-0.5)

    def start_of(i):
        return pl.multiple_of(jnp.minimum(i * chunk, units - chunk), 128)

    def remote(src, dst, send, recv, **where):
        return pltpu.make_async_remote_copy(
            src_ref=src, dst_ref=dst, send_sem=send, recv_sem=recv, device_id=where,
            device_id_type=MESH,
        )

    def landing(mat, src, half):
        if mat < 2:
            return (wg, wu)[mat].at[pl.ds(pl.multiple_of(src * depth + half * half_depth, half_depth), half_depth)]
        return wd.at[pl.ds(pl.multiple_of(half * half_chunk, half_chunk), half_chunk), pl.ds(pl.multiple_of(src * depth, depth), depth)]

    def weight_out(mat, dst):
        if mat < 2:
            src = (w_gate_ref, w_up_ref)[mat].at[pl.ds(pl.multiple_of(g * half_depth, half_depth), half_depth), pl.ds(start_of(dst), chunk)]
        else:
            src = w_down_ref.at[pl.ds(pl.multiple_of(start_of(dst) + g * half_chunk, math.gcd(128, half_chunk)), half_chunk)]
        return remote(src, landing(mat, s, g), wz_send.at[mat, dst], wz_recv.at[mat, s], sp=dst)

    def weight_in(mat, src):
        block = landing(mat, src, g)
        return remote(block, block, wz_send.at[mat, src], wz_recv.at[mat, src], sp=src)

    def weight_pass(mat, src, half):
        block = landing(mat, src, half)
        return remote(block, block, wy_send.at[mat, src], wy_recv.at[mat, src], grp=1 - g)

    def each(low, high, body):
        lax.fori_loop(low, high, lambda i, z: (body(i), z)[1], 0)

    def others(body):
        each(0, s, body)
        each(s + 1, ns, body)

    barrier = pltpu.get_barrier_semaphore()
    others(lambda i: pl.semaphore_signal(barrier, inc=1, device_id={"sp": i}, device_id_type=MESH))
    pl.semaphore_signal(barrier, inc=1, device_id={"grp": 1 - g}, device_id_type=MESH)
    for j in range(1, nt):
        pl.semaphore_signal(barrier, inc=1, device_id={"tp": (t + j) % nt}, device_id_type=MESH)
    pl.semaphore_wait(barrier, ns + nt - 1)

    def kv_out(i, kk, vv):
        return (
            remote(kk, kbuf.at[i], kv_send.at[0, i], kv_recv.at[0, i], sp=s + 1),
            remote(vv, vbuf.at[i], kv_send.at[1, i], kv_recv.at[1, i], sp=s + 1),
        )

    def kv_in(i):
        return (
            remote(kbuf.at[i], kbuf.at[i], kv_send.at[0, i], kv_recv.at[0, i], sp=s - 1),
            remote(vbuf.at[i], vbuf.at[i], kv_send.at[1, i], kv_recv.at[1, i], sp=s - 1),
        )

    @pl.when(s + 1 < ns)
    def _():
        for copy in kv_out(0, k_ref, v_ref):
            copy.start()

    def locals_():
        own = pl.ds(pl.multiple_of(s * depth, depth), depth)
        return (
            pltpu.make_async_copy(w_out_ref, w_out, loc_sem.at[0]),
            pltpu.make_async_copy(w_gate_ref.at[:, pl.ds(start_of(s), chunk)], wg.at[own], loc_sem.at[1]),
            pltpu.make_async_copy(w_up_ref.at[:, pl.ds(start_of(s), chunk)], wu.at[own], loc_sem.at[2]),
            pltpu.make_async_copy(w_down_ref.at[pl.ds(start_of(s), chunk)], wd.at[:, own], loc_sem.at[3]),
        )

    for copy in locals_():
        copy.start()
    for mat in range(3):
        each(0, s, lambda i, mat=mat: weight_out(mat, s - 1 - i).start())

    def start_up():
        for mat in range(3):
            each(s + 1, ns, lambda i, mat=mat: weight_out(mat, i).start())

    pl.when(s == 0)(start_up)

    gate_own = gate_ref[pl.ds(pl.multiple_of(s * tok, tok), tok), :]

    def attend(src, kk, vv, first):
        for h in range(nheads):
            lanes = slice(h * HEAD_DIM, (h + 1) * HEAD_DIM)
            scores = lax.dot_general(
                q_ref[:, lanes], kk[:, lanes], (((1,), (1,)), ((), ())), preferred_element_type=F32
            )
            key_gate = gate_t_ref[h : h + 1, pl.ds(pl.multiple_of(src * tok, tok), tok)]
            scores = scores * scale + gate_own[:, h : h + 1] - key_gate
            if first:
                row = lax.broadcasted_iota(jnp.int32, (tok, tok), 0)
                col = lax.broadcasted_iota(jnp.int32, (tok, tok), 1)
                scores = jnp.where(col <= row, scores, -1e30)
                new = jnp.max(scores, axis=-1, keepdims=True)
                w = jnp.where(col <= row, jnp.exp(scores - new), 0.0)
                tot[h] = jnp.sum(w, axis=-1, keepdims=True)
                acc[h] = jnp.dot(w.astype(BF16), vv[:, lanes], preferred_element_type=F32)
            else:
                old = top[h]
                new = jnp.maximum(old, jnp.max(scores, axis=-1, keepdims=True))
                w = jnp.exp(scores - new)
                shrink = jnp.exp(old - new)
                tot[h] = tot[h] * shrink + jnp.sum(w, axis=-1, keepdims=True)
                acc[h] = acc[h] * shrink + jnp.dot(
                    w.astype(BF16), vv[:, lanes], preferred_element_type=F32
                )
            top[h] = new

    attend(s, k_ref, v_ref, True)

    def earlier(i):
        for copy in kv_in(i - 1):
            copy.wait_recv()

        @pl.when(s + 1 < ns)
        def _():
            for copy in kv_out(i, kbuf.at[i - 1], vbuf.at[i - 1]):
                copy.start()

        pl.when(i == s)(start_up)
        attend(s - i, kbuf.at[i - 1], vbuf.at[i - 1], False)

    each(1, s + 1, earlier)

    for h in range(nheads):
        att[:, h * HEAD_DIM : (h + 1) * HEAD_DIM] = (acc[h] / tot[h]).astype(BF16)

    def head_copy(j):
        dst = (t + j) % nt
        return remote(
            att.at[pl.ds(pl.multiple_of(dst * rows, rows), rows)], heads.at[j - 1],
            h_send.at[j - 1], h_recv.at[j - 1], tp=dst,
        )

    for j in range(1, nt):
        head_copy(j).start()

    def pass_on(mat, src):
        weight_in(mat, src).wait_recv()
        weight_pass(mat, src, g).start()

    copies = locals_()
    copies[0].wait()
    resid[...] = resid_ref[...].astype(F32) + jnp.dot(
        att[pl.ds(pl.multiple_of(t * rows, rows), rows), :],
        w_out[pl.ds(pl.multiple_of(t * att_w, att_w), att_w), :], preferred_element_type=F32,
    )
    each(s + 1, ns, lambda i: pass_on(0, i))

    def mix(j):
        head_copy(j).wait_recv()
        src = (t + nt - j) % nt
        resid[...] += jnp.dot(
            heads[j - 1], w_out[pl.ds(pl.multiple_of(src * att_w, att_w), att_w), :],
            preferred_element_type=F32,
        )

    each(1, nt, mix)
    full = resid[...]
    normed = full * lax.rsqrt(jnp.mean(full * full, axis=-1, keepdims=True) + 1e-06)
    nall[s, t] = (normed * gain_ref[...]).astype(BF16)

    def row_z(side, src, to):
        block = nall.at[src, t]
        return remote(block, block, az_send.at[side, src], az_recv.at[side, src], sp=to)

    def row_x(src, who):
        block = nall.at[src, who]
        return remote(block, block, ax_send.at[src], ax_recv.at[src], tp=tx)

    def row_c(kind, src, who):
        block = nall.at[src, who]
        return remote(block, block, ac_send.at[kind, src], ac_recv.at[kind, src], tp=tc)

    def spread(src):
        row_x(src, t).start()
        row_c(0, src, t).start()

    def relay(src):
        row_x(src, tx).wait_recv()
        row_c(1, src, tx).start()

    pl.when(s + 1 < ns)(lambda: row_z(0, s, s + 1).start())
    pl.when(s > 0)(lambda: row_z(1, s, s - 1).start())
    spread(s)
    each(s + 1, ns, lambda i: pass_on(1, i))
    each(0, s, lambda i: pass_on(0, s - 1 - i))
    relay(s)
    each(s + 1, ns, lambda i: pass_on(2, i))
    each(0, s, lambda i: pass_on(1, s - 1 - i))
    each(0, s, lambda i: pass_on(2, s - 1 - i))

    def gather(d):
        @pl.when(s >= d)
        def _():
            row_z(0, s - d, s - 1).wait_recv()
            pl.when(s + 1 < ns)(lambda: row_z(0, s - d, s + 1).start())
            spread(s - d)

        @pl.when(s + d < ns)
        def _():
            row_z(1, s + d, s + 1).wait_recv()
            pl.when(s > 0)(lambda: row_z(1, s + d, s - 1).start())
            spread(s + d)

        @pl.when(d > 1)
        def _():
            pl.when(s >= d - 1)(lambda: relay(s - d + 1))
            pl.when(s + d - 1 < ns)(lambda: relay(s + d - 1))

    each(1, ns, gather)
    pl.when(s >= ns - 1)(lambda: relay(s - ns + 1))
    pl.when(s + ns - 1 < ns)(lambda: relay(s + ns - 1))

    for copy in copies[1:]:
        copy.wait()
    for mat in range(3):
        others(lambda i, mat=mat: weight_pass(mat, i, 1 - g).wait_recv())

    def rows_in(src):
        row_c(0, src, tc).wait_recv()
        row_c(1, src, (tc + 2) % 4).wait_recv()

    each(0, ns, rows_in)

    fresh = lax.broadcasted_iota(jnp.int32, (tok, chunk), 1) + start_of(s) >= s * chunk
    piece = math.gcd(width, 512)

    def sum_c(d):
        return remote(part.at[d, :, 1 - c], crecv.at[d], rc_send.at[d], rc_recv.at[d], tp=tc)

    def sum_x(d):
        return remote(csend.at[d], xrecv.at[d], rx_send.at[d], rx_recv.at[d], tp=tx)

    def sum_z(d):
        return remote(zsend.at[d], zrecv.at[d], rz_send.at[d], rz_recv.at[d], sp=(s + 1 + d) % ns)

    def stage_x(d):
        sum_c(d).wait_recv()
        csend[d] = (part[d, 1 - x, c].astype(F32) + crecv[d, 1 - x].astype(F32)).astype(BF16)
        sum_x(d).start()
        keep[d] = part[d, x, c].astype(F32) + crecv[d, x].astype(F32)

    def stage_z(d):
        sum_x(d).wait_recv()
        zsend[d] = (keep[d] + xrecv[d].astype(F32)).astype(BF16)
        sum_z(d).start()

    def feed(d):
        dst = (s + 1 + d) % ns
        a = nall[dst].reshape(tok, width)
        gate = jnp.dot(a, wg[...], preferred_element_type=F32)
        up = jnp.dot(a, wu[...], preferred_element_type=F32)
        hidden = jnp.where(fresh, gate / (1.0 + jnp.exp(-gate)) * up, 0.0).astype(BF16)

        def down(p):
            cols = pl.ds(pl.multiple_of(p * piece, piece), piece)
            y = jnp.dot(hidden, wd[:, cols], preferred_element_type=F32).astype(BF16)
            part[d, :, :, :, cols] = y.reshape(2, 2, rows, piece)

        each(0, width // piece, down)
        sum_c(d).start()
        pl.when(d >= 1)(lambda: stage_x(d - 1))
        pl.when(d >= 2)(lambda: stage_z(d - 2))

    each(0, ns, feed)
    stage_x(ns - 1)
    stage_z(ns - 2)
    sum_x(ns - 1).wait_recv()
    resid[...] += keep[ns - 1] + xrecv[ns - 1].astype(F32)

    def last(d):
        sum_z(d).wait_recv()
        resid[...] += zrecv[d].astype(F32)

    each(0, ns - 1, last)
    out_ref[...] = resid[...].astype(BF16)

    @pl.when(s + 1 < ns)
    def _():
        def sent(i):
            for copy in kv_out(i, kbuf.at[0], vbuf.at[0]):
                copy.wait_send()

        each(0, s + 1, sent)
        each(0, s + 1, lambda i: row_z(0, i, s + 1).wait_send())

    pl.when(s > 0)(lambda: each(s, ns, lambda i: row_z(1, i, s - 1).wait_send()))
    for mat in range(3):
        others(lambda i, mat=mat: weight_out(mat, i).wait_send())
        others(lambda i, mat=mat: weight_pass(mat, i, g).wait_send())
    for j in range(1, nt):
        head_copy(j).wait_send()

    def spread_done(i):
        row_x(i, t).wait_send()
        row_c(0, i, t).wait_send()
        row_c(1, i, tx).wait_send()
        sum_c(i).wait_send()
        sum_x(i).wait_send()

    each(0, ns, spread_done)
    each(0, ns - 1, lambda d: sum_z(d).wait_send())


def fused(ns, nt, chunk, resid_in, queries, keys, values, cum_gate, w_out, norm_gain, w_gate, w_up, w_down):
    rows, width = resid_in.shape
    tok, att_w = queries.shape
    depth, units = w_gate.shape
    nheads = att_w // HEAD_DIM
    vm = pl.BlockSpec(memory_space=pltpu.VMEM)
    hbm = pl.BlockSpec(memory_space=pltpu.HBM)
    dma = pltpu.SemaphoreType.DMA
    return pl.pallas_call(
        functools.partial(layer_kernel, (ns, nt, chunk)),
        out_shape=jax.ShapeDtypeStruct((rows, width), BF16),
        in_specs=[vm] * 7 + [hbm] * 4,
        out_specs=vm,
        scratch_shapes=[
            pltpu.VMEM((ns - 1, tok, att_w), BF16),
            pltpu.VMEM((ns - 1, tok, att_w), BF16),
            pltpu.VMEM((nheads, tok, 1), F32),
            pltpu.VMEM((nheads, tok, 1), F32),
            pltpu.VMEM((nheads, tok, HEAD_DIM), F32),
            pltpu.VMEM((tok, att_w), BF16),
            pltpu.VMEM((nt - 1, rows, att_w), BF16),
            pltpu.VMEM(w_out.shape, BF16),
            pltpu.VMEM((rows, width), F32),
            pltpu.VMEM((ns, nt, rows, width), BF16),
            pltpu.VMEM((width, chunk), BF16),
            pltpu.VMEM((width, chunk), BF16),
            pltpu.VMEM((chunk, width), BF16),
            pltpu.VMEM((ns, 2, 2, rows, width), BF16),
            pltpu.VMEM((ns, 2, rows, width), BF16),
            pltpu.VMEM((ns, rows, width), BF16),
            pltpu.VMEM((ns, rows, width), F32),
            pltpu.VMEM((ns, rows, width), BF16),
            pltpu.VMEM((ns, rows, width), BF16),
            pltpu.VMEM((ns, rows, width), BF16),
            dma((4,)),
            dma((2, ns)), dma((2, ns)),
            dma((3, ns)), dma((3, ns)),
            dma((3, ns)), dma((3, ns)),
            dma((nt - 1,)), dma((nt - 1,)),
            dma((2, ns)), dma((2, ns)),
            dma((ns,)), dma((ns,)),
            dma((2, ns)), dma((2, ns)),
            dma((ns,)), dma((ns,)),
            dma((ns,)), dma((ns,)),
            dma((ns,)), dma((ns,)),
        ],
        compiler_params=pltpu.CompilerParams(
            collective_id=0, has_side_effects=True, vmem_limit_bytes=60 * 2**20
        ),
        name="layer",
    )(
        resid_in, queries, keys, values, cum_gate, cum_gate.T, norm_gain[None, :], w_out, w_gate,
        w_up, w_down,
    )


def pick(mesh):
    ng, ns, nt = (mesh.shape[a] for a in ("grp", "sp", "tp"))

    def step(*args):
        resid_in, queries, cum_gate, w_gate = args[0], args[1], args[4], args[7]
        rows, width = resid_in.shape
        depth, units = w_gate.shape
        chunk = -(-units // (128 * ns)) * 128
        need = 2 * ns * nt * rows * width * 4 + 6 * width * chunk + 2 * args[5].size
        fits = (
            ng == 2 and nt == 4 and ns > 1 and units % 128 == 0 and (ns - 1) * chunk < units
            and depth % 256 == 0 and width == ns * depth and rows % 16 == 0
            and queries.shape[0] == rows * nt and queries.shape[0] % 128 == 0
            and cum_gate.shape[0] == ns * nt * rows and queries.shape[1] % 128 == 0
            and need < 40 * 2**20
        )
        if fits:
            return fused(ns, nt, chunk, *args)
        return on_device(*args)

    return step


def solution(mesh):
    return jax.shard_map(
        pick(mesh),
        mesh=mesh,
        in_specs=(
            P(("grp", "sp", "tp"), None),
            P(("grp", "sp"), "tp"),
            P(("grp", "sp"), "tp"),
            P(("grp", "sp"), "tp"),
            P("grp", "tp"),
            P(),
            P(),
            P("sp", "tp"),
            P("sp", "tp"),
            P("tp", "sp"),
        ),
        out_specs=P(("grp", "sp", "tp"), None),
        check_vma=False,
    )
```

```python
import functools
import math

import jax
import jax.numpy as jnp
from jax import lax
from jax.experimental import pallas as pl
from jax.experimental.pallas import tpu as pltpu
from jax.sharding import PartitionSpec as P

HEAD_DIM = 64


def on_device(resid_in, queries, keys, values, cum_gate, w_out, norm_gain, w_gate, w_up, w_down):
    tok_rows = queries.shape[0]
    local_heads = queries.shape[1] // HEAD_DIM
    scale = HEAD_DIM ** (-0.5)
    offset = lax.axis_index("sp") * tok_rows
    query_heads = queries.reshape(tok_rows, local_heads, HEAD_DIM)
    own_gate = lax.dynamic_slice_in_dim(cum_gate, offset, tok_rows, 0).T
    query_pos = offset + jnp.arange(tok_rows, dtype=jnp.int32)
    last_pos = offset + tok_rows - 1
    initial = (
        jnp.full((local_heads, tok_rows), -1e30, jnp.float32),
        jnp.zeros((local_heads, tok_rows), jnp.float32),
        jnp.zeros((tok_rows, local_heads, HEAD_DIM), jnp.float32),
    )
    pair = lax.all_gather(jnp.stack([keys, values]), "sp", axis=1, tiled=True)
    key_piece, value_piece = pair[0], pair[1]
    length = key_piece.shape[0]
    span = math.gcd(length, 512)

    def block(index, state):
        begin = index * span

        def work(inner):
            maxima, totals, summed = inner
            key_block = lax.dynamic_slice_in_dim(key_piece, index * span, span, 0).reshape(
                span, local_heads, HEAD_DIM
            )
            value_block_rows = lax.dynamic_slice_in_dim(value_piece, index * span, span, 0).reshape(
                span, local_heads, HEAD_DIM
            )
            key_gate = lax.dynamic_slice_in_dim(cum_gate, begin, span, 0).T
            scores = (
                jnp.einsum(
                    "qhd,khd->hqk", query_heads, key_block, preferred_element_type=jnp.float32
                )
                * scale
            )
            scores = scores + own_gate[:, :, None] - key_gate[:, None, :]
            key_pos = begin + jnp.arange(span, dtype=jnp.int32)
            mask = (key_pos[None, :] <= query_pos[:, None])[None]
            scores = jnp.where(mask, scores, -1e30)
            new_max = jnp.maximum(maxima, jnp.max(scores, axis=-1))
            weights = jnp.where(mask, jnp.exp(scores - new_max[:, :, None]), 0.0)
            rescale = jnp.exp(maxima - new_max)
            totals = totals * rescale + jnp.sum(weights, axis=-1)
            product = jnp.einsum(
                "hqk,khd->qhd",
                weights.astype(jnp.bfloat16),
                value_block_rows,
                preferred_element_type=jnp.float32,
            )
            summed = summed * rescale.T[:, :, None] + product
            return (new_max, totals, summed)

        return lax.cond(begin <= last_pos, work, lambda inner: inner, state)

    maxima, totals, summed = lax.fori_loop(0, length // span, block, initial)
    attended = (
        (summed / totals.T[:, :, None])
        .reshape(tok_rows, local_heads * HEAD_DIM)
        .astype(jnp.bfloat16)
    )
    head_rows = lax.all_to_all(attended, "tp", split_axis=0, concat_axis=1, tiled=True)
    mixed = jnp.dot(head_rows, w_out, preferred_element_type=jnp.float32)
    resid = resid_in.astype(jnp.float32) + mixed
    normed = resid * lax.rsqrt(jnp.mean(resid * resid, axis=-1, keepdims=True) + 1e-06)
    normed = (normed * norm_gain).astype(jnp.bfloat16)
    all_rows = lax.all_gather(normed, ("sp", "tp"), axis=0, tiled=True)
    full_gate, full_up, full_down = (
        lax.all_to_all(w_gate, "sp", split_axis=1, concat_axis=0, tiled=True),
        lax.all_to_all(w_up, "sp", split_axis=1, concat_axis=0, tiled=True),
        lax.all_to_all(w_down, "sp", split_axis=0, concat_axis=1, tiled=True),
    )
    gate = jnp.dot(all_rows, full_gate, preferred_element_type=jnp.float32)
    up = jnp.dot(all_rows, full_up, preferred_element_type=jnp.float32)
    hidden = (jax.nn.silu(gate) * up).astype(jnp.bfloat16)
    terms = jnp.dot(hidden, full_down, preferred_element_type=jnp.float32)
    back = lax.psum_scatter(
        terms.astype(jnp.bfloat16), ("sp", "tp"), scatter_dimension=0, tiled=True
    ).astype(jnp.float32)
    return (resid + back).astype(jnp.bfloat16)


MESH = pl.DeviceIdType.MESH
F32 = jnp.float32
BF16 = jnp.bfloat16


def layer_kernel(
    dims, resid_ref, q_ref, k_ref, v_ref, gate_ref, gate_t_ref, gain_ref, w_out_ref, w_gate_ref,
    w_up_ref, w_down_ref, out_ref, kbuf, vbuf, top, tot, acc, att, heads, w_out, resid, nall, wg,
    wu, wd, part, crecv, csend, keep, xrecv, zsend, zrecv, loc_sem, kv_send, kv_recv, wz_send,
    wz_recv, wy_send, wy_recv, h_send, h_recv, az_send, az_recv, ax_send, ax_recv, ac_send,
    ac_recv, rc_send, rc_recv, rx_send, rx_recv, rz_send, rz_recv, go,
):
    ns, nt, chunk = dims
    g, s, t = lax.axis_index("grp"), lax.axis_index("sp"), lax.axis_index("tp")
    rows, width = resid_ref.shape
    tok, att_w = q_ref.shape
    depth, units = w_gate_ref.shape
    nheads = att_w // HEAD_DIM
    half_depth = depth // 2
    dup = ns * chunk - units
    x, c = t // 2, t % 2
    tx = (t + 2) % 4
    tc = t + 1 - 2 * c
    scale = HEAD_DIM ** (-0.5)

    def start_of(i):
        return pl.multiple_of(jnp.minimum(i * chunk, units - chunk), 128)

    def remote(src, dst, send, recv, **where):
        return pltpu.make_async_remote_copy(
            src_ref=src, dst_ref=dst, send_sem=send, recv_sem=recv, device_id=where,
            device_id_type=MESH,
        )

    def xor(a, b):
        hi, lo, bh, bl = a // 2, a % 2, b // 2, b % 2
        return 2 * (hi + bh - 2 * hi * bh) + lo + bl - 2 * lo * bl

    def landing(mat, src, half, skip):
        if mat < 2:
            return (wg, wu)[mat].at[
                pl.ds(pl.multiple_of(src * depth + half * half_depth, half_depth), half_depth),
                pl.ds(skip, chunk - skip),
            ]
        size = (chunk - skip) // 2
        return wd.at[
            pl.ds(pl.multiple_of(skip + half * size, math.gcd(128, size)), size),
            pl.ds(pl.multiple_of(src * depth, depth), depth),
        ]

    def weight_out(mat, dst, skip):
        if mat < 2:
            src = (w_gate_ref, w_up_ref)[mat].at[
                pl.ds(pl.multiple_of(g * half_depth, half_depth), half_depth),
                pl.ds(pl.multiple_of(start_of(dst) + skip, 128), chunk - skip),
            ]
        else:
            size = (chunk - skip) // 2
            src = w_down_ref.at[
                pl.ds(pl.multiple_of(start_of(dst) + skip + g * size, math.gcd(128, size)), size)
            ]
        return remote(
            src, landing(mat, s, g, skip), wz_send.at[mat, dst], wz_recv.at[mat, s], sp=dst
        )

    def weight_in(mat, src, skip):
        block = landing(mat, src, g, skip)
        return remote(block, block, wz_send.at[mat, src], wz_recv.at[mat, src], sp=src)

    def weight_pass(mat, src, half, skip):
        block = landing(mat, src, half, skip)
        return remote(block, block, wy_send.at[mat, src], wy_recv.at[mat, src], grp=1 - g)

    def sized(dst, body):
        pl.when(dst < ns - 1)(lambda: body(0))
        pl.when(dst == ns - 1)(lambda: body(dup))

    def each(low, high, body):
        lax.fori_loop(low, high, lambda i, z: (body(i), z)[1], 0)

    def others(body):
        each(0, s, body)
        each(s + 1, ns, body)

    barrier = pltpu.get_barrier_semaphore()
    others(lambda i: pl.semaphore_signal(barrier, inc=1, device_id={"sp": i}, device_id_type=MESH))
    pl.semaphore_signal(barrier, inc=1, device_id={"grp": 1 - g}, device_id_type=MESH)
    for j in range(1, nt):
        pl.semaphore_signal(barrier, inc=1, device_id={"tp": (t + j) % nt}, device_id_type=MESH)
    pl.semaphore_wait(barrier, ns + nt - 1)

    def kv_out(i, kk, vv):
        return (
            remote(kk, kbuf.at[i], kv_send.at[0, i], kv_recv.at[0, i], sp=s + 1),
            remote(vv, vbuf.at[i], kv_send.at[1, i], kv_recv.at[1, i], sp=s + 1),
        )

    def kv_in(i):
        return (
            remote(kbuf.at[i], kbuf.at[i], kv_send.at[0, i], kv_recv.at[0, i], sp=s - 1),
            remote(vbuf.at[i], vbuf.at[i], kv_send.at[1, i], kv_recv.at[1, i], sp=s - 1),
        )

    @pl.when(s + 1 < ns)
    def _():
        for copy in kv_out(0, k_ref, v_ref):
            copy.start()

    def locals_():
        own = pl.ds(pl.multiple_of(s * depth, depth), depth)
        return (
            pltpu.make_async_copy(w_out_ref, w_out, loc_sem.at[0]),
            pltpu.make_async_copy(w_gate_ref.at[:, pl.ds(start_of(s), chunk)], wg.at[own], loc_sem.at[1]),
            pltpu.make_async_copy(w_up_ref.at[:, pl.ds(start_of(s), chunk)], wu.at[own], loc_sem.at[2]),
            pltpu.make_async_copy(w_down_ref.at[pl.ds(start_of(s), chunk)], wd.at[:, own], loc_sem.at[3]),
        )

    for copy in locals_():
        copy.start()
    def send_weight(mat, dst):
        sized(dst, lambda skip: weight_out(mat, dst, skip).start())

    for mat in range(2):
        each(0, s, lambda i, mat=mat: send_weight(mat, s - 1 - i))

    if dup:

        @pl.when(s == ns - 1)
        def _():
            for mat in range(2):
                def clear(i, mat=mat):
                    band = pl.ds(pl.multiple_of((i + (i >= s)) * depth, depth), depth)
                    (wg, wu)[mat][band, :dup] = jnp.zeros((depth, dup), BF16)

                each(0, ns - 1, clear)
            wd[:dup, : (ns - 1) * depth] = jnp.zeros((dup, (ns - 1) * depth), BF16)

    gate_own = gate_ref[pl.ds(pl.multiple_of(s * tok, tok), tok), :]

    def attend(src, kk, vv, first):
        for h in range(nheads):
            lanes = slice(h * HEAD_DIM, (h + 1) * HEAD_DIM)
            scores = lax.dot_general(
                q_ref[:, lanes], kk[:, lanes], (((1,), (1,)), ((), ())), preferred_element_type=F32
            )
            key_gate = gate_t_ref[h : h + 1, pl.ds(pl.multiple_of(src * tok, tok), tok)]
            scores = scores * scale + gate_own[:, h : h + 1] - key_gate
            if first:
                row = lax.broadcasted_iota(jnp.int32, (tok, tok), 0)
                col = lax.broadcasted_iota(jnp.int32, (tok, tok), 1)
                scores = jnp.where(col <= row, scores, -1e30)
                new = jnp.max(scores, axis=-1, keepdims=True)
                w = jnp.where(col <= row, jnp.exp(scores - new), 0.0)
                tot[h] = jnp.sum(w, axis=-1, keepdims=True)
                acc[h] = jnp.dot(w.astype(BF16), vv[:, lanes], preferred_element_type=F32)
            else:
                old = top[h]
                new = jnp.maximum(old, jnp.max(scores, axis=-1, keepdims=True))
                w = jnp.exp(scores - new)
                shrink = jnp.exp(old - new)
                tot[h] = tot[h] * shrink + jnp.sum(w, axis=-1, keepdims=True)
                acc[h] = acc[h] * shrink + jnp.dot(
                    w.astype(BF16), vv[:, lanes], preferred_element_type=F32
                )
            top[h] = new

    attend(s, k_ref, v_ref, True)

    def earlier(i):
        for copy in kv_in(i - 1):
            copy.wait_recv()

        @pl.when(s + 1 < ns)
        def _():
            for copy in kv_out(i, kbuf.at[i - 1], vbuf.at[i - 1]):
                copy.start()

        @pl.when((i == s) & (s == ns - 2))
        def _():
            each(
                0, s,
                lambda j: pl.semaphore_signal(
                    go, inc=1, device_id={"sp": j}, device_id_type=MESH
                ),
            )

        attend(s - i, kbuf.at[i - 1], vbuf.at[i - 1], False)

    each(1, s + 1, earlier)

    for h in range(nheads):
        att[:, h * HEAD_DIM : (h + 1) * HEAD_DIM] = (acc[h] / tot[h]).astype(BF16)

    def head_copy(j):
        dst = (t + j) % nt
        return remote(
            att.at[pl.ds(pl.multiple_of(dst * rows, rows), rows)], heads.at[j - 1],
            h_send.at[j - 1], h_recv.at[j - 1], tp=dst,
        )

    for j in range(1, nt):
        head_copy(j).start()

    def pass_on(mat, src):
        def body(skip):
            weight_in(mat, src, skip).wait_recv()
            weight_pass(mat, src, g, skip).start()

        sized(s, body)

    copies = locals_()
    copies[0].wait()
    resid[...] = resid_ref[...].astype(F32) + jnp.dot(
        att[pl.ds(pl.multiple_of(t * rows, rows), rows), :],
        w_out[pl.ds(pl.multiple_of(t * att_w, att_w), att_w), :], preferred_element_type=F32,
    )

    def mix(j):
        head_copy(j).wait_recv()
        src = (t + nt - j) % nt
        resid[...] += jnp.dot(
            heads[j - 1], w_out[pl.ds(pl.multiple_of(src * att_w, att_w), att_w), :],
            preferred_element_type=F32,
        )

    each(1, nt, mix)
    full = resid[...]
    normed = full * lax.rsqrt(jnp.mean(full * full, axis=-1, keepdims=True) + 1e-06)
    nall[s, t] = (normed * gain_ref[...]).astype(BF16)

    def row_z(src, to):
        block = nall.at[src, t]
        return remote(block, block, az_send.at[0, src], az_recv.at[src], sp=to)

    def row_far(to):
        block = nall.at[s, t]
        return remote(block, block, az_send.at[1, s], az_recv.at[s], sp=to)

    def row_x(src, who):
        block = nall.at[src, who]
        return remote(block, block, ax_send.at[src], ax_recv.at[src], tp=tx)

    def row_c(kind, src, who):
        block = nall.at[src, who]
        return remote(block, block, ac_send.at[kind, src], ac_recv.at[kind, src], tp=tc)

    def spread(src):
        row_x(src, t).start()
        row_c(0, src, t).start()

    def relay(src):
        row_x(src, tx).wait_recv()
        row_c(1, src, tx).start()

    near, far, cross = xor(s, 1), xor(s, 2), xor(s, 3)
    pl.when(s < ns - 2)(lambda: pl.semaphore_wait(go, 1))
    row_far(far).start()
    row_z(s, near).start()
    for mat in range(2):
        each(s + 1, ns, lambda i, mat=mat: send_weight(mat, i))
    each(0, s, lambda i: send_weight(2, s - 1 - i))
    each(s + 1, ns, lambda i: send_weight(2, i))
    spread(s)

    def take_far():
        row_z(far, far).wait_recv()
        row_z(far, near).start()
        spread(far)

    def take(src):
        row_z(src, near).wait_recv()
        spread(src)

    for mat in range(2):
        each(s + 1, ns, lambda i, mat=mat: pass_on(mat, i))
    relay(s)
    pl.when(s >= 2)(take_far)
    for mat in range(2):
        each(0, s, lambda i, mat=mat: pass_on(mat, s - 1 - i))
    pl.when(s < 2)(take_far)
    take(near)
    relay(far)
    take(cross)
    relay(near)
    each(s + 1, ns, lambda i: pass_on(2, i))
    each(0, s, lambda i: pass_on(2, s - 1 - i))
    relay(cross)

    for copy in copies[1:]:
        copy.wait()
    for mat in range(3):
        others(lambda i, mat=mat: sized(s, lambda skip: weight_pass(mat, i, 1 - g, skip).wait_recv()))

    def rows_in(src):
        row_c(0, src, tc).wait_recv()
        row_c(1, src, (tc + 2) % 4).wait_recv()

    each(0, ns, rows_in)

    fresh = lax.broadcasted_iota(jnp.int32, (tok, chunk), 1) + start_of(s) >= s * chunk
    piece = math.gcd(width, 512)

    def sum_c(d):
        return remote(part.at[d, :, 1 - c], crecv.at[d], rc_send.at[d], rc_recv.at[d], tp=tc)

    def sum_x(d):
        return remote(csend.at[d], xrecv.at[d], rx_send.at[d], rx_recv.at[d], tp=tx)

    def sum_z(d):
        return remote(zsend.at[d], zrecv.at[d], rz_send.at[d], rz_recv.at[d], sp=xor(s, 1 + d % 2))

    def stage_x(d):
        sum_c(d).wait_recv()
        csend[d] = (part[d, 1 - x, c].astype(F32) + crecv[d, 1 - x].astype(F32)).astype(BF16)
        sum_x(d).start()
        keep[d] = part[d, x, c].astype(F32) + crecv[d, x].astype(F32)

    def stage_z(d):
        sum_x(d).wait_recv()
        keep[d] = keep[d] + xrecv[d].astype(F32)

        @pl.when(d == 1)
        def _():
            sum_z(0).wait_recv()
            keep[1] = keep[1] + zrecv[0].astype(F32)

        zsend[d] = keep[d].astype(BF16)
        sum_z(d).start()

    def feed(d):
        dst = xor(s, 3 - d)
        a = nall[dst].reshape(tok, width)
        gate = jnp.dot(a, wg[...], preferred_element_type=F32)
        up = jnp.dot(a, wu[...], preferred_element_type=F32)
        hidden = jnp.where(fresh, gate / (1.0 + jnp.exp(-gate)) * up, 0.0).astype(BF16)

        def down(p):
            cols = pl.ds(pl.multiple_of(p * piece, piece), piece)
            y = jnp.dot(hidden, wd[:, cols], preferred_element_type=F32).astype(BF16)
            part[d, :, :, :, cols] = y.reshape(2, 2, rows, piece)

        each(0, width // piece, down)
        sum_c(d).start()
        pl.when(d >= 1)(lambda: stage_x(d - 1))
        pl.when(d >= 2)(lambda: stage_z(d - 2))

    each(0, ns, feed)
    stage_x(ns - 1)
    stage_z(ns - 2)
    sum_x(ns - 1).wait_recv()
    resid[...] += keep[ns - 1] + xrecv[ns - 1].astype(F32)

    for d in (1, 2):
        sum_z(d).wait_recv()
        resid[...] += zrecv[d].astype(F32)
    out_ref[...] = resid[...].astype(BF16)

    @pl.when(s + 1 < ns)
    def _():
        def sent(i):
            for copy in kv_out(i, kbuf.at[0], vbuf.at[0]):
                copy.wait_send()

        each(0, s + 1, sent)

    row_far(far).wait_send()
    row_z(s, near).wait_send()
    row_z(far, near).wait_send()
    for mat in range(3):
        others(lambda i, mat=mat: sized(i, lambda skip: weight_out(mat, i, skip).wait_send()))
        others(lambda i, mat=mat: sized(s, lambda skip: weight_pass(mat, i, g, skip).wait_send()))
    for j in range(1, nt):
        head_copy(j).wait_send()

    def spread_done(i):
        row_x(i, t).wait_send()
        row_c(0, i, t).wait_send()
        row_c(1, i, tx).wait_send()
        sum_c(i).wait_send()
        sum_x(i).wait_send()

    each(0, ns, spread_done)
    each(0, ns - 1, lambda d: sum_z(d).wait_send())


def fused(ns, nt, chunk, resid_in, queries, keys, values, cum_gate, w_out, norm_gain, w_gate, w_up, w_down):
    rows, width = resid_in.shape
    tok, att_w = queries.shape
    depth, units = w_gate.shape
    nheads = att_w // HEAD_DIM
    vm = pl.BlockSpec(memory_space=pltpu.VMEM)
    hbm = pl.BlockSpec(memory_space=pltpu.HBM)
    dma = pltpu.SemaphoreType.DMA
    return pl.pallas_call(
        functools.partial(layer_kernel, (ns, nt, chunk)),
        out_shape=jax.ShapeDtypeStruct((rows, width), BF16),
        in_specs=[vm] * 7 + [hbm] * 4,
        out_specs=vm,
        scratch_shapes=[
            pltpu.VMEM((ns - 1, tok, att_w), BF16),
            pltpu.VMEM((ns - 1, tok, att_w), BF16),
            pltpu.VMEM((nheads, tok, 1), F32),
            pltpu.VMEM((nheads, tok, 1), F32),
            pltpu.VMEM((nheads, tok, HEAD_DIM), F32),
            pltpu.VMEM((tok, att_w), BF16),
            pltpu.VMEM((nt - 1, rows, att_w), BF16),
            pltpu.VMEM(w_out.shape, BF16),
            pltpu.VMEM((rows, width), F32),
            pltpu.VMEM((ns, nt, rows, width), BF16),
            pltpu.VMEM((width, chunk), BF16),
            pltpu.VMEM((width, chunk), BF16),
            pltpu.VMEM((chunk, width), BF16),
            pltpu.VMEM((ns, 2, 2, rows, width), BF16),
            pltpu.VMEM((ns, 2, rows, width), BF16),
            pltpu.VMEM((ns, rows, width), BF16),
            pltpu.VMEM((ns, rows, width), F32),
            pltpu.VMEM((ns, rows, width), BF16),
            pltpu.VMEM((ns, rows, width), BF16),
            pltpu.VMEM((ns, rows, width), BF16),
            dma((4,)),
            dma((2, ns)), dma((2, ns)),
            dma((3, ns)), dma((3, ns)),
            dma((3, ns)), dma((3, ns)),
            dma((nt - 1,)), dma((nt - 1,)),
            dma((2, ns)), dma((ns,)),
            dma((ns,)), dma((ns,)),
            dma((2, ns)), dma((2, ns)),
            dma((ns,)), dma((ns,)),
            dma((ns,)), dma((ns,)),
            dma((ns,)), dma((ns,)),
            pltpu.SemaphoreType.REGULAR,
        ],
        compiler_params=pltpu.CompilerParams(
            collective_id=0, has_side_effects=True, vmem_limit_bytes=60 * 2**20
        ),
        name="layer",
    )(
        resid_in, queries, keys, values, cum_gate, cum_gate.T, norm_gain[None, :], w_out, w_gate,
        w_up, w_down,
    )


def pick(mesh):
    ng, ns, nt = (mesh.shape[a] for a in ("grp", "sp", "tp"))

    def step(*args):
        resid_in, queries, cum_gate, w_gate = args[0], args[1], args[4], args[7]
        rows, width = resid_in.shape
        depth, units = w_gate.shape
        chunk = -(-units // (128 * ns)) * 128
        need = 2 * ns * nt * rows * width * 4 + 6 * width * chunk + 2 * args[5].size
        fits = (
            ng == 2 and nt == 4 and ns == 4 and units % 128 == 0 and (ns - 1) * chunk < units
            and depth % 256 == 0 and (chunk - ns * chunk + units) % 32 == 0 and width == ns * depth and rows % 16 == 0
            and queries.shape[0] == rows * nt and queries.shape[0] % 128 == 0
            and cum_gate.shape[0] == ns * nt * rows and queries.shape[1] % 128 == 0
            and need < 40 * 2**20
        )
        if fits:
            return fused(ns, nt, chunk, *args)
        return on_device(*args)

    return step


def solution(mesh):
    return jax.shard_map(
        pick(mesh),
        mesh=mesh,
        in_specs=(
            P(("grp", "sp", "tp"), None),
            P(("grp", "sp"), "tp"),
            P(("grp", "sp"), "tp"),
            P(("grp", "sp"), "tp"),
            P("grp", "tp"),
            P(),
            P(),
            P("sp", "tp"),
            P("sp", "tp"),
            P("tp", "sp"),
        ),
        out_specs=P(("grp", "sp", "tp"), None),
        check_vma=False,
    )
```

```python
import functools
import math

import jax
import jax.numpy as jnp
from jax import lax
from jax.experimental import pallas as pl
from jax.experimental.pallas import tpu as pltpu
from jax.sharding import PartitionSpec as P

HEAD_DIM = 64


def on_device(resid_in, queries, keys, values, cum_gate, w_out, norm_gain, w_gate, w_up, w_down):
    tok_rows = queries.shape[0]
    local_heads = queries.shape[1] // HEAD_DIM
    scale = HEAD_DIM ** (-0.5)
    offset = lax.axis_index("sp") * tok_rows
    query_heads = queries.reshape(tok_rows, local_heads, HEAD_DIM)
    own_gate = lax.dynamic_slice_in_dim(cum_gate, offset, tok_rows, 0).T
    query_pos = offset + jnp.arange(tok_rows, dtype=jnp.int32)
    last_pos = offset + tok_rows - 1
    initial = (
        jnp.full((local_heads, tok_rows), -1e30, jnp.float32),
        jnp.zeros((local_heads, tok_rows), jnp.float32),
        jnp.zeros((tok_rows, local_heads, HEAD_DIM), jnp.float32),
    )
    pair = lax.all_gather(jnp.stack([keys, values]), "sp", axis=1, tiled=True)
    key_piece, value_piece = pair[0], pair[1]
    length = key_piece.shape[0]
    span = math.gcd(length, 512)

    def block(index, state):
        begin = index * span

        def work(inner):
            maxima, totals, summed = inner
            key_block = lax.dynamic_slice_in_dim(key_piece, index * span, span, 0).reshape(
                span, local_heads, HEAD_DIM
            )
            value_block_rows = lax.dynamic_slice_in_dim(value_piece, index * span, span, 0).reshape(
                span, local_heads, HEAD_DIM
            )
            key_gate = lax.dynamic_slice_in_dim(cum_gate, begin, span, 0).T
            scores = (
                jnp.einsum(
                    "qhd,khd->hqk", query_heads, key_block, preferred_element_type=jnp.float32
                )
                * scale
            )
            scores = scores + own_gate[:, :, None] - key_gate[:, None, :]
            key_pos = begin + jnp.arange(span, dtype=jnp.int32)
            mask = (key_pos[None, :] <= query_pos[:, None])[None]
            scores = jnp.where(mask, scores, -1e30)
            new_max = jnp.maximum(maxima, jnp.max(scores, axis=-1))
            weights = jnp.where(mask, jnp.exp(scores - new_max[:, :, None]), 0.0)
            rescale = jnp.exp(maxima - new_max)
            totals = totals * rescale + jnp.sum(weights, axis=-1)
            product = jnp.einsum(
                "hqk,khd->qhd",
                weights.astype(jnp.bfloat16),
                value_block_rows,
                preferred_element_type=jnp.float32,
            )
            summed = summed * rescale.T[:, :, None] + product
            return (new_max, totals, summed)

        return lax.cond(begin <= last_pos, work, lambda inner: inner, state)

    maxima, totals, summed = lax.fori_loop(0, length // span, block, initial)
    attended = (
        (summed / totals.T[:, :, None])
        .reshape(tok_rows, local_heads * HEAD_DIM)
        .astype(jnp.bfloat16)
    )
    head_rows = lax.all_to_all(attended, "tp", split_axis=0, concat_axis=1, tiled=True)
    mixed = jnp.dot(head_rows, w_out, preferred_element_type=jnp.float32)
    resid = resid_in.astype(jnp.float32) + mixed
    normed = resid * lax.rsqrt(jnp.mean(resid * resid, axis=-1, keepdims=True) + 1e-06)
    normed = (normed * norm_gain).astype(jnp.bfloat16)
    all_rows = lax.all_gather(normed, ("sp", "tp"), axis=0, tiled=True)
    full_gate, full_up, full_down = (
        lax.all_to_all(w_gate, "sp", split_axis=1, concat_axis=0, tiled=True),
        lax.all_to_all(w_up, "sp", split_axis=1, concat_axis=0, tiled=True),
        lax.all_to_all(w_down, "sp", split_axis=0, concat_axis=1, tiled=True),
    )
    gate = jnp.dot(all_rows, full_gate, preferred_element_type=jnp.float32)
    up = jnp.dot(all_rows, full_up, preferred_element_type=jnp.float32)
    hidden = (jax.nn.silu(gate) * up).astype(jnp.bfloat16)
    terms = jnp.dot(hidden, full_down, preferred_element_type=jnp.float32)
    back = lax.psum_scatter(
        terms.astype(jnp.bfloat16), ("sp", "tp"), scatter_dimension=0, tiled=True
    ).astype(jnp.float32)
    return (resid + back).astype(jnp.bfloat16)


MESH = pl.DeviceIdType.MESH
F32 = jnp.float32
BF16 = jnp.bfloat16


def layer_kernel(
    dims, resid_ref, q_ref, k_ref, v_ref, gate_t_ref, gain_ref, w_out_ref, w_gate_ref,
    w_up_ref, w_down_ref, out_ref, kbuf, vbuf, top, tot, acc, att, heads, w_out, resid, nall, wg,
    wu, wd, hidden, part, crecv, csend, keep, xrecv, zsend, zrecv, loc_sem, kv_send, kv_recv, wz_send,
    wz_recv, wy_send, wy_recv, h_send, h_recv, az_send, az_recv, ax_send, ax_recv, ac_send,
    ac_recv, rc_send, rc_recv, rx_send, rx_recv, rz_send, rz_recv, go,
):
    ns, nt, chunk = dims
    g, s, t = lax.axis_index("grp"), lax.axis_index("sp"), lax.axis_index("tp")
    rows, width = resid_ref.shape
    tok, att_w = q_ref.shape
    depth, units = w_gate_ref.shape
    nheads = att_w // HEAD_DIM
    half_depth = depth // 2
    dup = ns * chunk - units
    x, c = t // 2, t % 2
    tx = (t + 2) % 4
    tc = t + 1 - 2 * c
    scale = HEAD_DIM ** (-0.5)

    def start_of(i):
        return pl.multiple_of(jnp.minimum(i * chunk, units - chunk), 128)

    def remote(src, dst, send, recv, **where):
        return pltpu.make_async_remote_copy(
            src_ref=src, dst_ref=dst, send_sem=send, recv_sem=recv, device_id=where,
            device_id_type=MESH,
        )

    def xor(a, b):
        hi, lo, bh, bl = a // 2, a % 2, b // 2, b % 2
        return 2 * (hi + bh - 2 * hi * bh) + lo + bl - 2 * lo * bl

    def landing(mat, src, half, skip):
        if mat < 2:
            return (wg, wu)[mat].at[
                pl.ds(pl.multiple_of(src * depth + half * half_depth, half_depth), half_depth),
                pl.ds(skip, chunk - skip),
            ]
        size = (chunk - skip) // 2
        return wd.at[
            pl.ds(pl.multiple_of(skip + half * size, math.gcd(128, size)), size),
            pl.ds(pl.multiple_of(src * depth, depth), depth),
        ]

    def weight_out(mat, dst, skip):
        if mat < 2:
            src = (w_gate_ref, w_up_ref)[mat].at[
                pl.ds(pl.multiple_of(g * half_depth, half_depth), half_depth),
                pl.ds(pl.multiple_of(start_of(dst) + skip, 128), chunk - skip),
            ]
        else:
            size = (chunk - skip) // 2
            src = w_down_ref.at[
                pl.ds(pl.multiple_of(start_of(dst) + skip + g * size, math.gcd(128, size)), size)
            ]
        return remote(
            src, landing(mat, s, g, skip), wz_send.at[mat, dst], wz_recv.at[mat, s], sp=dst
        )

    def weight_in(mat, src, skip):
        block = landing(mat, src, g, skip)
        return remote(block, block, wz_send.at[mat, src], wz_recv.at[mat, src], sp=src)

    def weight_pass(mat, src, half, skip):
        block = landing(mat, src, half, skip)
        return remote(block, block, wy_send.at[mat, src], wy_recv.at[mat, src], grp=1 - g)

    def sized(dst, body):
        pl.when(dst < ns - 1)(lambda: body(0))
        pl.when(dst == ns - 1)(lambda: body(dup))

    def each(low, high, body):
        lax.fori_loop(low, high, lambda i, z: (body(i), z)[1], 0)

    def others(body):
        each(0, s, body)
        each(s + 1, ns, body)

    barrier = pltpu.get_barrier_semaphore()
    others(lambda i: pl.semaphore_signal(barrier, inc=1, device_id={"sp": i}, device_id_type=MESH))
    pl.semaphore_signal(barrier, inc=1, device_id={"grp": 1 - g}, device_id_type=MESH)
    for j in range(1, nt):
        pl.semaphore_signal(barrier, inc=1, device_id={"tp": (t + j) % nt}, device_id_type=MESH)
    pl.semaphore_wait(barrier, ns + nt - 1)

    def kv_out(i, kk, vv):
        return (
            remote(kk, kbuf.at[i], kv_send.at[0, i], kv_recv.at[0, i], sp=s + 1),
            remote(vv, vbuf.at[i], kv_send.at[1, i], kv_recv.at[1, i], sp=s + 1),
        )

    def kv_in(i):
        return (
            remote(kbuf.at[i], kbuf.at[i], kv_send.at[0, i], kv_recv.at[0, i], sp=s - 1),
            remote(vbuf.at[i], vbuf.at[i], kv_send.at[1, i], kv_recv.at[1, i], sp=s - 1),
        )

    @pl.when(s + 1 < ns)
    def _():
        for copy in kv_out(0, k_ref, v_ref):
            copy.start()

    def locals_():
        own = pl.ds(pl.multiple_of(s * depth, depth), depth)
        return (
            pltpu.make_async_copy(w_out_ref, w_out, loc_sem.at[0]),
            pltpu.make_async_copy(w_gate_ref.at[:, pl.ds(start_of(s), chunk)], wg.at[own], loc_sem.at[1]),
            pltpu.make_async_copy(w_up_ref.at[:, pl.ds(start_of(s), chunk)], wu.at[own], loc_sem.at[2]),
            pltpu.make_async_copy(w_down_ref.at[pl.ds(start_of(s), chunk)], wd.at[:, own], loc_sem.at[3]),
        )

    for copy in locals_():
        copy.start()
    def send_weight(mat, dst):
        sized(dst, lambda skip: weight_out(mat, dst, skip).start())

    for mat in range(2):
        each(0, s, lambda i, mat=mat: send_weight(mat, s - 1 - i))

    if dup:

        @pl.when(s == ns - 1)
        def _():
            for mat in range(2):
                def clear(i, mat=mat):
                    band = pl.ds(pl.multiple_of((i + (i >= s)) * depth, depth), depth)
                    (wg, wu)[mat][band, :dup] = jnp.zeros((depth, dup), BF16)

                each(0, ns - 1, clear)
            wd[:dup, : (ns - 1) * depth] = jnp.zeros((dup, (ns - 1) * depth), BF16)

    gate_own = gate_t_ref[:, pl.ds(pl.multiple_of(s * tok, tok), tok)].T

    def attend(src, kk, vv, first):
        for h in range(nheads):
            lanes = slice(h * HEAD_DIM, (h + 1) * HEAD_DIM)
            scores = lax.dot_general(
                q_ref[:, lanes], kk[:, lanes], (((1,), (1,)), ((), ())), preferred_element_type=F32
            )
            key_gate = gate_t_ref[h : h + 1, pl.ds(pl.multiple_of(src * tok, tok), tok)]
            scores = scores * scale + gate_own[:, h : h + 1] - key_gate
            if first:
                row = lax.broadcasted_iota(jnp.int32, (tok, tok), 0)
                col = lax.broadcasted_iota(jnp.int32, (tok, tok), 1)
                scores = jnp.where(col <= row, scores, -1e30)
                new = jnp.max(scores, axis=-1, keepdims=True)
                w = jnp.where(col <= row, jnp.exp(scores - new), 0.0)
                tot[h] = jnp.sum(w, axis=-1, keepdims=True)
                acc[h] = jnp.dot(w.astype(BF16), vv[:, lanes], preferred_element_type=F32)
            else:
                old = top[h]
                new = jnp.maximum(old, jnp.max(scores, axis=-1, keepdims=True))
                w = jnp.exp(scores - new)
                shrink = jnp.exp(old - new)
                tot[h] = tot[h] * shrink + jnp.sum(w, axis=-1, keepdims=True)
                acc[h] = acc[h] * shrink + jnp.dot(
                    w.astype(BF16), vv[:, lanes], preferred_element_type=F32
                )
            top[h] = new

    attend(s, k_ref, v_ref, True)

    def earlier(i):
        for copy in kv_in(i - 1):
            copy.wait_recv()

        @pl.when(s + 1 < ns)
        def _():
            for copy in kv_out(i, kbuf.at[i - 1], vbuf.at[i - 1]):
                copy.start()

        @pl.when((i == s) & (s == ns - 2))
        def _():
            each(
                0, s,
                lambda j: pl.semaphore_signal(
                    go, inc=1, device_id={"sp": j}, device_id_type=MESH
                ),
            )

        attend(s - i, kbuf.at[i - 1], vbuf.at[i - 1], False)

    each(1, s + 1, earlier)

    for h in range(nheads):
        att[:, h * HEAD_DIM : (h + 1) * HEAD_DIM] = (acc[h] / tot[h]).astype(BF16)

    def head_copy(j):
        dst = (t + j) % nt
        return remote(
            att.at[pl.ds(pl.multiple_of(dst * rows, rows), rows)], heads.at[j - 1],
            h_send.at[j - 1], h_recv.at[j - 1], tp=dst,
        )

    for j in range(1, nt):
        head_copy(j).start()

    def pass_on(mat, src):
        def body(skip):
            weight_in(mat, src, skip).wait_recv()
            weight_pass(mat, src, g, skip).start()

        sized(s, body)

    copies = locals_()
    copies[0].wait()
    resid[...] = resid_ref[...].astype(F32) + jnp.dot(
        att[pl.ds(pl.multiple_of(t * rows, rows), rows), :],
        w_out[pl.ds(pl.multiple_of(t * att_w, att_w), att_w), :], preferred_element_type=F32,
    )

    def mix(j):
        head_copy(j).wait_recv()
        src = (t + nt - j) % nt
        resid[...] += jnp.dot(
            heads[j - 1], w_out[pl.ds(pl.multiple_of(src * att_w, att_w), att_w), :],
            preferred_element_type=F32,
        )

    each(1, nt, mix)
    full = resid[...]
    normed = full * lax.rsqrt(jnp.mean(full * full, axis=-1, keepdims=True) + 1e-06)
    nall[s, t] = (normed * gain_ref[...]).astype(BF16)

    def row_z(src, to):
        block = nall.at[src, t]
        return remote(block, block, az_send.at[0, src], az_recv.at[src], sp=to)

    def row_far(to):
        block = nall.at[s, t]
        return remote(block, block, az_send.at[1, s], az_recv.at[s], sp=to)

    def row_x(src, who):
        block = nall.at[src, who]
        return remote(block, block, ax_send.at[src], ax_recv.at[src], tp=tx)

    def row_c(kind, src, who):
        block = nall.at[src, who]
        return remote(block, block, ac_send.at[kind, src], ac_recv.at[kind, src], tp=tc)

    def spread(src):
        row_x(src, t).start()
        row_c(0, src, t).start()

    def relay(src):
        row_x(src, tx).wait_recv()
        row_c(1, src, tx).start()

    near, far, cross = xor(s, 1), xor(s, 2), xor(s, 3)
    pl.when(s < ns - 2)(lambda: pl.semaphore_wait(go, 1))
    row_far(far).start()
    row_z(s, near).start()
    for mat in range(2):
        each(s + 1, ns, lambda i, mat=mat: send_weight(mat, i))
    each(0, s, lambda i: send_weight(2, s - 1 - i))
    each(s + 1, ns, lambda i: send_weight(2, i))
    spread(s)

    def take_far():
        row_z(far, far).wait_recv()
        row_z(far, near).start()
        spread(far)

    def take(src):
        row_z(src, near).wait_recv()
        spread(src)

    for mat in range(2):
        each(s + 1, ns, lambda i, mat=mat: pass_on(mat, i))
    relay(s)
    pl.when(s >= 2)(take_far)
    for mat in range(2):
        each(0, s, lambda i, mat=mat: pass_on(mat, s - 1 - i))
    pl.when(s < 2)(take_far)
    take(near)
    relay(far)
    take(cross)
    relay(near)

    for copy in copies[1:]:
        copy.wait()

    def twin_in(mat):
        others(lambda i: sized(s, lambda skip: weight_pass(mat, i, 1 - g, skip).wait_recv()))

    twin_in(0)
    twin_in(1)
    fresh = lax.broadcasted_iota(jnp.int32, (tok, chunk), 1) + start_of(s) >= s * chunk
    half = width // 2
    piece = math.gcd(half, 512)

    def hide(src):
        row_c(0, src, tc).wait_recv()
        row_c(1, src, (tc + 2) % 4).wait_recv()
        a = nall[src].reshape(tok, width)
        gate = jnp.dot(a, wg[...], preferred_element_type=F32)
        up = jnp.dot(a, wu[...], preferred_element_type=F32)
        hidden[src] = jnp.where(fresh, gate / (1.0 + jnp.exp(-gate)) * up, 0.0).astype(BF16)

    each(0, ns - 1, lambda k: hide(xor(s, k)))
    each(s + 1, ns, lambda i: pass_on(2, i))
    each(0, s, lambda i: pass_on(2, s - 1 - i))
    relay(cross)
    hide(cross)
    twin_in(2)

    def sum_c(d):
        return remote(part.at[d, :, 1 - c], crecv.at[d], rc_send.at[d], rc_recv.at[d], tp=tc)

    def sum_x(d):
        return remote(csend.at[d], xrecv.at[d], rx_send.at[d], rx_recv.at[d], tp=tx)

    def sum_z(d):
        return remote(zsend.at[d], zrecv.at[d], rz_send.at[d], rz_recv.at[d], sp=xor(s, 1 + d // 2 % 2))

    def stage_x(d):
        sum_c(d).wait_recv()
        csend[d] = (part[d, 1 - x, c].astype(F32) + crecv[d, 1 - x].astype(F32)).astype(BF16)
        sum_x(d).start()
        keep[d] = part[d, x, c].astype(F32) + crecv[d, x].astype(F32)

    def stage_z(d):
        sum_x(d).wait_recv()
        keep[d] = keep[d] + xrecv[d].astype(F32)

        @pl.when((d == 2) | (d == 3))
        def _():
            sum_z(d - 2).wait_recv()
            keep[d] = keep[d] + zrecv[d - 2].astype(F32)

        zsend[d] = keep[d].astype(BF16)
        sum_z(d).start()

    def feed(d):
        src = hidden[xor(s, 3 - d // 2)]

        def down(p):
            cols = pl.ds(pl.multiple_of(p * piece, piece), piece)
            from_ = pl.ds(pl.multiple_of(d % 2 * half + p * piece, piece), piece)
            y = jnp.dot(src, wd[:, from_], preferred_element_type=F32).astype(BF16)
            part[d, :, :, :, cols] = y.reshape(2, 2, rows, piece)

        each(0, half // piece, down)
        sum_c(d).start()
        pl.when(d >= 1)(lambda: stage_x(d - 1))
        pl.when(d >= 3)(lambda: stage_z(d - 3))

    each(0, 2 * ns, feed)
    stage_x(2 * ns - 1)
    stage_z(2 * ns - 3)
    for d in (6, 7):
        cols = slice((d - 6) * half, (d - 5) * half)
        sum_x(d).wait_recv()
        sum_z(d - 4).wait_recv()
        sum_z(d - 2).wait_recv()
        resid[:, cols] += (
            keep[d] + xrecv[d].astype(F32) + zrecv[d - 4].astype(F32) + zrecv[d - 2].astype(F32)
        )
    out_ref[...] = resid[...].astype(BF16)

    @pl.when(s + 1 < ns)
    def _():
        def sent(i):
            for copy in kv_out(i, kbuf.at[0], vbuf.at[0]):
                copy.wait_send()

        each(0, s + 1, sent)

    row_far(far).wait_send()
    row_z(s, near).wait_send()
    row_z(far, near).wait_send()
    for mat in range(3):
        others(lambda i, mat=mat: sized(i, lambda skip: weight_out(mat, i, skip).wait_send()))
        others(lambda i, mat=mat: sized(s, lambda skip: weight_pass(mat, i, g, skip).wait_send()))
    for j in range(1, nt):
        head_copy(j).wait_send()

    def spread_done(i):
        row_x(i, t).wait_send()
        row_c(0, i, t).wait_send()
        row_c(1, i, tx).wait_send()

    each(0, ns, spread_done)

    def sums_done(d):
        sum_c(d).wait_send()
        sum_x(d).wait_send()

    each(0, 2 * ns, sums_done)
    each(0, 2 * ns - 2, lambda d: sum_z(d).wait_send())


def fused(ns, nt, chunk, resid_in, queries, keys, values, cum_gate, w_out, norm_gain, w_gate, w_up, w_down):
    rows, width = resid_in.shape
    tok, att_w = queries.shape
    depth, units = w_gate.shape
    nheads = att_w // HEAD_DIM
    vm = pl.BlockSpec(memory_space=pltpu.VMEM)
    hbm = pl.BlockSpec(memory_space=pltpu.HBM)
    dma = pltpu.SemaphoreType.DMA
    return pl.pallas_call(
        functools.partial(layer_kernel, (ns, nt, chunk)),
        out_shape=jax.ShapeDtypeStruct((rows, width), BF16),
        in_specs=[vm] * 6 + [hbm] * 4,
        out_specs=vm,
        scratch_shapes=[
            pltpu.VMEM((ns - 1, tok, att_w), BF16),
            pltpu.VMEM((ns - 1, tok, att_w), BF16),
            pltpu.VMEM((nheads, tok, 1), F32),
            pltpu.VMEM((nheads, tok, 1), F32),
            pltpu.VMEM((nheads, tok, HEAD_DIM), F32),
            pltpu.VMEM((tok, att_w), BF16),
            pltpu.VMEM((nt - 1, rows, att_w), BF16),
            pltpu.VMEM(w_out.shape, BF16),
            pltpu.VMEM((rows, width), F32),
            pltpu.VMEM((ns, nt, rows, width), BF16),
            pltpu.VMEM((width, chunk), BF16),
            pltpu.VMEM((width, chunk), BF16),
            pltpu.VMEM((chunk, width), BF16),
            pltpu.VMEM((ns, tok, chunk), BF16),
            pltpu.VMEM((2 * ns, 2, 2, rows, width // 2), BF16),
            pltpu.VMEM((2 * ns, 2, rows, width // 2), BF16),
            pltpu.VMEM((2 * ns, rows, width // 2), BF16),
            pltpu.VMEM((2 * ns, rows, width // 2), F32),
            pltpu.VMEM((2 * ns, rows, width // 2), BF16),
            pltpu.VMEM((2 * ns, rows, width // 2), BF16),
            pltpu.VMEM((2 * ns, rows, width // 2), BF16),
            dma((4,)),
            dma((2, ns)), dma((2, ns)),
            dma((3, ns)), dma((3, ns)),
            dma((3, ns)), dma((3, ns)),
            dma((nt - 1,)), dma((nt - 1,)),
            dma((2, ns)), dma((ns,)),
            dma((ns,)), dma((ns,)),
            dma((2, ns)), dma((2, ns)),
            dma((2 * ns,)), dma((2 * ns,)),
            dma((2 * ns,)), dma((2 * ns,)),
            dma((2 * ns,)), dma((2 * ns,)),
            pltpu.SemaphoreType.REGULAR,
        ],
        compiler_params=pltpu.CompilerParams(
            collective_id=0, has_side_effects=True, vmem_limit_bytes=60 * 2**20
        ),
        name="layer",
    )(
        resid_in, queries, keys, values, cum_gate.T, norm_gain[None, :], w_out, w_gate,
        w_up, w_down,
    )


def pick(mesh):
    ng, ns, nt = (mesh.shape[a] for a in ("grp", "sp", "tp"))

    def step(*args):
        resid_in, queries, cum_gate, w_gate = args[0], args[1], args[4], args[7]
        rows, width = resid_in.shape
        depth, units = w_gate.shape
        chunk = -(-units // (128 * ns)) * 128
        need = 2 * ns * nt * rows * width * 4 + 6 * width * chunk + 2 * args[5].size
        fits = (
            ng == 2 and nt == 4 and ns == 4 and units % 128 == 0 and (ns - 1) * chunk < units
            and depth % 256 == 0 and width % 256 == 0 and (chunk - ns * chunk + units) % 32 == 0 and width == ns * depth and rows % 16 == 0
            and queries.shape[0] == rows * nt and queries.shape[0] % 128 == 0
            and cum_gate.shape[0] == ns * nt * rows and queries.shape[1] % 128 == 0
            and need < 40 * 2**20
        )
        if fits:
            return fused(ns, nt, chunk, *args)
        return on_device(*args)

    return step


def solution(mesh):
    return jax.shard_map(
        pick(mesh),
        mesh=mesh,
        in_specs=(
            P(("grp", "sp", "tp"), None),
            P(("grp", "sp"), "tp"),
            P(("grp", "sp"), "tp"),
            P(("grp", "sp"), "tp"),
            P("grp", "tp"),
            P(),
            P(),
            P("sp", "tp"),
            P("sp", "tp"),
            P("tp", "sp"),
        ),
        out_specs=P(("grp", "sp", "tp"), None),
        check_vma=False,
    )
```

```python
import functools
import math

import jax
import jax.numpy as jnp
from jax import lax
from jax.experimental import pallas as pl
from jax.experimental.pallas import tpu as pltpu
from jax.sharding import PartitionSpec as P

HEAD_DIM = 64


def on_device(resid_in, queries, keys, values, cum_gate, w_out, norm_gain, w_gate, w_up, w_down):
    tok_rows = queries.shape[0]
    local_heads = queries.shape[1] // HEAD_DIM
    scale = HEAD_DIM ** (-0.5)
    offset = lax.axis_index("sp") * tok_rows
    query_heads = queries.reshape(tok_rows, local_heads, HEAD_DIM)
    own_gate = lax.dynamic_slice_in_dim(cum_gate, offset, tok_rows, 0).T
    query_pos = offset + jnp.arange(tok_rows, dtype=jnp.int32)
    last_pos = offset + tok_rows - 1
    initial = (
        jnp.full((local_heads, tok_rows), -1e30, jnp.float32),
        jnp.zeros((local_heads, tok_rows), jnp.float32),
        jnp.zeros((tok_rows, local_heads, HEAD_DIM), jnp.float32),
    )
    pair = lax.all_gather(jnp.stack([keys, values]), "sp", axis=1, tiled=True)
    key_piece, value_piece = pair[0], pair[1]
    length = key_piece.shape[0]
    span = math.gcd(length, 512)

    def block(index, state):
        begin = index * span

        def work(inner):
            maxima, totals, summed = inner
            key_block = lax.dynamic_slice_in_dim(key_piece, index * span, span, 0).reshape(
                span, local_heads, HEAD_DIM
            )
            value_block_rows = lax.dynamic_slice_in_dim(value_piece, index * span, span, 0).reshape(
                span, local_heads, HEAD_DIM
            )
            key_gate = lax.dynamic_slice_in_dim(cum_gate, begin, span, 0).T
            scores = (
                jnp.einsum(
                    "qhd,khd->hqk", query_heads, key_block, preferred_element_type=jnp.float32
                )
                * scale
            )
            scores = scores + own_gate[:, :, None] - key_gate[:, None, :]
            key_pos = begin + jnp.arange(span, dtype=jnp.int32)
            mask = (key_pos[None, :] <= query_pos[:, None])[None]
            scores = jnp.where(mask, scores, -1e30)
            new_max = jnp.maximum(maxima, jnp.max(scores, axis=-1))
            weights = jnp.where(mask, jnp.exp(scores - new_max[:, :, None]), 0.0)
            rescale = jnp.exp(maxima - new_max)
            totals = totals * rescale + jnp.sum(weights, axis=-1)
            product = jnp.einsum(
                "hqk,khd->qhd",
                weights.astype(jnp.bfloat16),
                value_block_rows,
                preferred_element_type=jnp.float32,
            )
            summed = summed * rescale.T[:, :, None] + product
            return (new_max, totals, summed)

        return lax.cond(begin <= last_pos, work, lambda inner: inner, state)

    maxima, totals, summed = lax.fori_loop(0, length // span, block, initial)
    attended = (
        (summed / totals.T[:, :, None])
        .reshape(tok_rows, local_heads * HEAD_DIM)
        .astype(jnp.bfloat16)
    )
    head_rows = lax.all_to_all(attended, "tp", split_axis=0, concat_axis=1, tiled=True)
    mixed = jnp.dot(head_rows, w_out, preferred_element_type=jnp.float32)
    resid = resid_in.astype(jnp.float32) + mixed
    normed = resid * lax.rsqrt(jnp.mean(resid * resid, axis=-1, keepdims=True) + 1e-06)
    normed = (normed * norm_gain).astype(jnp.bfloat16)
    all_rows = lax.all_gather(normed, ("sp", "tp"), axis=0, tiled=True)
    full_gate, full_up, full_down = (
        lax.all_to_all(w_gate, "sp", split_axis=1, concat_axis=0, tiled=True),
        lax.all_to_all(w_up, "sp", split_axis=1, concat_axis=0, tiled=True),
        lax.all_to_all(w_down, "sp", split_axis=0, concat_axis=1, tiled=True),
    )
    gate = jnp.dot(all_rows, full_gate, preferred_element_type=jnp.float32)
    up = jnp.dot(all_rows, full_up, preferred_element_type=jnp.float32)
    hidden = (jax.nn.silu(gate) * up).astype(jnp.bfloat16)
    terms = jnp.dot(hidden, full_down, preferred_element_type=jnp.float32)
    back = lax.psum_scatter(
        terms.astype(jnp.bfloat16), ("sp", "tp"), scatter_dimension=0, tiled=True
    ).astype(jnp.float32)
    return (resid + back).astype(jnp.bfloat16)


MESH = pl.DeviceIdType.MESH
F32 = jnp.float32
BF16 = jnp.bfloat16


def layer_kernel(
    dims, resid_ref, q_ref, k_ref, v_ref, gate_t_ref, gain_ref, w_out_ref, w_gate_ref,
    w_up_ref, w_down_ref, out_ref, kbuf, vbuf, top, tot, acc, att, heads, w_out, resid, nall, wg,
    wu, wd, hidden, part, crecv, csend, keep, xrecv, zsend, zrecv, loc_sem, kv_send, kv_recv, wz_send,
    wz_recv, wy_send, wy_recv, h_send, h_recv, az_send, az_recv, ax_send, ax_recv, ac_send,
    ac_recv, rc_send, rc_recv, rx_send, rx_recv, rz_send, rz_recv, go,
):
    ns, nt, chunk = dims
    g, s, t = lax.axis_index("grp"), lax.axis_index("sp"), lax.axis_index("tp")
    rows, width = resid_ref.shape
    tok, att_w = q_ref.shape
    depth, units = w_gate_ref.shape
    nheads = att_w // HEAD_DIM
    half_depth = depth // 2
    dup = ns * chunk - units
    x, c = t // 2, t % 2
    tx = (t + 2) % 4
    tc = t + 1 - 2 * c
    scale = HEAD_DIM ** (-0.5)

    def start_of(i):
        return pl.multiple_of(jnp.minimum(i * chunk, units - chunk), 128)

    def remote(src, dst, send, recv, **where):
        return pltpu.make_async_remote_copy(
            src_ref=src, dst_ref=dst, send_sem=send, recv_sem=recv, device_id=where,
            device_id_type=MESH,
        )

    def xor(a, b):
        hi, lo, bh, bl = a // 2, a % 2, b // 2, b % 2
        return 2 * (hi + bh - 2 * hi * bh) + lo + bl - 2 * lo * bl

    def landing(mat, src, half, skip):
        if mat < 2:
            return (wg, wu)[mat].at[
                pl.ds(pl.multiple_of(src * depth + half * half_depth, half_depth), half_depth),
                pl.ds(skip, chunk - skip),
            ]
        size = (chunk - skip) // 2
        return wd.at[
            pl.ds(pl.multiple_of(skip + half * size, math.gcd(128, size)), size),
            pl.ds(pl.multiple_of(src * depth, depth), depth),
        ]

    def weight_out(mat, dst, skip):
        if mat < 2:
            src = (w_gate_ref, w_up_ref)[mat].at[
                pl.ds(pl.multiple_of(g * half_depth, half_depth), half_depth),
                pl.ds(pl.multiple_of(start_of(dst) + skip, 128), chunk - skip),
            ]
        else:
            size = (chunk - skip) // 2
            src = w_down_ref.at[
                pl.ds(pl.multiple_of(start_of(dst) + skip + g * size, math.gcd(128, size)), size)
            ]
        return remote(
            src, landing(mat, s, g, skip), wz_send.at[mat, dst], wz_recv.at[mat, s], sp=dst
        )

    def weight_in(mat, src, skip):
        block = landing(mat, src, g, skip)
        return remote(block, block, wz_send.at[mat, src], wz_recv.at[mat, src], sp=src)

    def weight_pass(mat, src, half, skip):
        block = landing(mat, src, half, skip)
        return remote(block, block, wy_send.at[mat, src], wy_recv.at[mat, src], grp=1 - g)

    def sized(dst, body):
        pl.when(dst < ns - 1)(lambda: body(0))
        pl.when(dst == ns - 1)(lambda: body(dup))

    def each(low, high, body):
        lax.fori_loop(low, high, lambda i, z: (body(i), z)[1], 0)

    def others(body):
        each(0, s, body)
        each(s + 1, ns, body)

    barrier = pltpu.get_barrier_semaphore()
    others(lambda i: pl.semaphore_signal(barrier, inc=1, device_id={"sp": i}, device_id_type=MESH))
    pl.semaphore_signal(barrier, inc=1, device_id={"grp": 1 - g}, device_id_type=MESH)
    for j in range(1, nt):
        pl.semaphore_signal(barrier, inc=1, device_id={"tp": (t + j) % nt}, device_id_type=MESH)
    pl.semaphore_wait(barrier, ns + nt - 1)

    def kv_out(i, kk, vv):
        return (
            remote(kk, kbuf.at[i], kv_send.at[0, i], kv_recv.at[0, i], sp=s + 1),
            remote(vv, vbuf.at[i], kv_send.at[1, i], kv_recv.at[1, i], sp=s + 1),
        )

    def kv_in(i):
        return (
            remote(kbuf.at[i], kbuf.at[i], kv_send.at[0, i], kv_recv.at[0, i], sp=s - 1),
            remote(vbuf.at[i], vbuf.at[i], kv_send.at[1, i], kv_recv.at[1, i], sp=s - 1),
        )

    @pl.when(s + 1 < ns)
    def _():
        for copy in kv_out(0, k_ref, v_ref):
            copy.start()

    def locals_():
        own = pl.ds(pl.multiple_of(s * depth, depth), depth)
        return (
            pltpu.make_async_copy(w_out_ref, w_out, loc_sem.at[0]),
            pltpu.make_async_copy(w_gate_ref.at[:, pl.ds(start_of(s), chunk)], wg.at[own], loc_sem.at[1]),
            pltpu.make_async_copy(w_up_ref.at[:, pl.ds(start_of(s), chunk)], wu.at[own], loc_sem.at[2]),
            pltpu.make_async_copy(w_down_ref.at[pl.ds(start_of(s), chunk)], wd.at[:, own], loc_sem.at[3]),
        )

    for copy in locals_():
        copy.start()
    def send_weight(mat, dst):
        sized(dst, lambda skip: weight_out(mat, dst, skip).start())

    each(0, s, lambda i: send_weight(0, s - 1 - i))

    if dup:

        @pl.when(s == ns - 1)
        def _():
            for mat in range(2):
                def clear(i, mat=mat):
                    band = pl.ds(pl.multiple_of((i + (i >= s)) * depth, depth), depth)
                    (wg, wu)[mat][band, :dup] = jnp.zeros((depth, dup), BF16)

                each(0, ns - 1, clear)
            wd[:dup, : (ns - 1) * depth] = jnp.zeros((dup, (ns - 1) * depth), BF16)

    gate_own = gate_t_ref[:, pl.ds(pl.multiple_of(s * tok, tok), tok)].T

    def attend(src, kk, vv, first):
        for h in range(nheads):
            lanes = slice(h * HEAD_DIM, (h + 1) * HEAD_DIM)
            scores = lax.dot_general(
                q_ref[:, lanes], kk[:, lanes], (((1,), (1,)), ((), ())), preferred_element_type=F32
            )
            key_gate = gate_t_ref[h : h + 1, pl.ds(pl.multiple_of(src * tok, tok), tok)]
            scores = scores * scale + gate_own[:, h : h + 1] - key_gate
            if first:
                row = lax.broadcasted_iota(jnp.int32, (tok, tok), 0)
                col = lax.broadcasted_iota(jnp.int32, (tok, tok), 1)
                scores = jnp.where(col <= row, scores, -1e30)
                new = jnp.max(scores, axis=-1, keepdims=True)
                w = jnp.where(col <= row, jnp.exp(scores - new), 0.0)
                tot[h] = jnp.sum(w, axis=-1, keepdims=True)
                acc[h] = jnp.dot(w.astype(BF16), vv[:, lanes], preferred_element_type=F32)
            else:
                old = top[h]
                new = jnp.maximum(old, jnp.max(scores, axis=-1, keepdims=True))
                w = jnp.exp(scores - new)
                shrink = jnp.exp(old - new)
                tot[h] = tot[h] * shrink + jnp.sum(w, axis=-1, keepdims=True)
                acc[h] = acc[h] * shrink + jnp.dot(
                    w.astype(BF16), vv[:, lanes], preferred_element_type=F32
                )
            top[h] = new

    attend(s, k_ref, v_ref, True)

    def earlier(i):
        for copy in kv_in(i - 1):
            copy.wait_recv()

        @pl.when(s + 1 < ns)
        def _():
            for copy in kv_out(i, kbuf.at[i - 1], vbuf.at[i - 1]):
                copy.start()

        @pl.when((i == s) & (s == ns - 2))
        def _():
            each(
                0, s,
                lambda j: pl.semaphore_signal(
                    go, inc=1, device_id={"sp": j}, device_id_type=MESH
                ),
            )

        attend(s - i, kbuf.at[i - 1], vbuf.at[i - 1], False)

    each(1, s + 1, earlier)

    for h in range(nheads):
        att[:, h * HEAD_DIM : (h + 1) * HEAD_DIM] = (acc[h] / tot[h]).astype(BF16)

    def head_copy(j):
        dst = (t + j) % nt
        return remote(
            att.at[pl.ds(pl.multiple_of(dst * rows, rows), rows)], heads.at[j - 1],
            h_send.at[j - 1], h_recv.at[j - 1], tp=dst,
        )

    for j in range(1, nt):
        head_copy(j).start()

    def pass_on(mat, src):
        def body(skip):
            weight_in(mat, src, skip).wait_recv()
            weight_pass(mat, src, g, skip).start()

        sized(s, body)

    copies = locals_()
    copies[0].wait()
    resid[...] = resid_ref[...].astype(F32) + jnp.dot(
        att[pl.ds(pl.multiple_of(t * rows, rows), rows), :],
        w_out[pl.ds(pl.multiple_of(t * att_w, att_w), att_w), :], preferred_element_type=F32,
    )

    def mix(j):
        head_copy(j).wait_recv()
        src = (t + nt - j) % nt
        resid[...] += jnp.dot(
            heads[j - 1], w_out[pl.ds(pl.multiple_of(src * att_w, att_w), att_w), :],
            preferred_element_type=F32,
        )

    each(1, nt, mix)
    full = resid[...]
    normed = full * lax.rsqrt(jnp.mean(full * full, axis=-1, keepdims=True) + 1e-06)
    nall[s, t] = (normed * gain_ref[...]).astype(BF16)

    def row_z(src, to):
        block = nall.at[src, t]
        return remote(block, block, az_send.at[0, src], az_recv.at[src], sp=to)

    def row_far(to):
        block = nall.at[s, t]
        return remote(block, block, az_send.at[1, s], az_recv.at[s], sp=to)

    def row_x(src, who):
        block = nall.at[src, who]
        return remote(block, block, ax_send.at[src], ax_recv.at[src], tp=tx)

    def row_c(kind, src, who):
        block = nall.at[src, who]
        return remote(block, block, ac_send.at[kind, src], ac_recv.at[kind, src], tp=tc)

    def spread(src):
        row_x(src, t).start()
        row_c(0, src, t).start()

    def relay(src):
        row_x(src, tx).wait_recv()
        row_c(1, src, tx).start()

    near, far, cross = xor(s, 1), xor(s, 2), xor(s, 3)
    pl.when(s < ns - 2)(lambda: pl.semaphore_wait(go, 1))
    row_far(far).start()
    row_z(s, near).start()
    for mat in range(3):
        each(s + 1, ns, lambda i, mat=mat: send_weight(mat, i))
        if mat:
            each(0, s, lambda i, mat=mat: send_weight(mat, s - 1 - i))
    spread(s)

    def take_far():
        row_z(far, far).wait_recv()
        row_z(far, near).start()
        spread(far)

    def take(src):
        row_z(src, near).wait_recv()
        spread(src)

    def pass_all(mat):
        each(s + 1, ns, lambda i: pass_on(mat, i))
        each(0, s, lambda i: pass_on(mat, s - 1 - i))

    each(s + 1, ns, lambda i: pass_on(0, i))
    relay(s)
    take_far()
    take(near)
    relay(far)
    take(cross)
    relay(near)
    each(0, s, lambda i: pass_on(0, s - 1 - i))
    relay(cross)
    pass_all(1)
    for copy in copies[1:]:
        copy.wait()

    def twin_in(mat):
        others(lambda i: sized(s, lambda skip: weight_pass(mat, i, 1 - g, skip).wait_recv()))

    twin_in(0)
    twin_in(1)
    fresh = lax.broadcasted_iota(jnp.int32, (tok, chunk), 1) + start_of(s) >= s * chunk
    half = width // 2
    piece = math.gcd(half, 512)

    def hide(src):
        row_c(0, src, tc).wait_recv()
        row_c(1, src, (tc + 2) % 4).wait_recv()
        a = nall[src].reshape(tok, width)
        gate = jnp.dot(a, wg[...], preferred_element_type=F32)
        up = jnp.dot(a, wu[...], preferred_element_type=F32)
        hidden[src] = jnp.where(fresh, gate / (1.0 + jnp.exp(-gate)) * up, 0.0).astype(BF16)

    each(0, ns, lambda k: hide(xor(s, k)))
    pass_all(2)
    twin_in(2)

    def sum_c(d):
        return remote(part.at[d, :, 1 - c], crecv.at[d], rc_send.at[d], rc_recv.at[d], tp=tc)

    def sum_x(d):
        return remote(csend.at[d], xrecv.at[d], rx_send.at[d], rx_recv.at[d], tp=tx)

    def sum_z(d):
        return remote(zsend.at[d], zrecv.at[d], rz_send.at[d], rz_recv.at[d], sp=xor(s, 1 + d // 2 % 2))

    def stage_x(d):
        sum_c(d).wait_recv()
        csend[d] = (part[d, 1 - x, c].astype(F32) + crecv[d, 1 - x].astype(F32)).astype(BF16)
        sum_x(d).start()
        keep[d] = part[d, x, c].astype(F32) + crecv[d, x].astype(F32)

    def stage_z(d):
        sum_x(d).wait_recv()
        keep[d] = keep[d] + xrecv[d].astype(F32)

        @pl.when((d == 2) | (d == 3))
        def _():
            sum_z(d - 2).wait_recv()
            keep[d] = keep[d] + zrecv[d - 2].astype(F32)

        zsend[d] = keep[d].astype(BF16)
        sum_z(d).start()

    def feed(d):
        src = hidden[xor(s, 3 - d // 2)]

        def down(p):
            cols = pl.ds(pl.multiple_of(p * piece, piece), piece)
            from_ = pl.ds(pl.multiple_of(d % 2 * half + p * piece, piece), piece)
            y = jnp.dot(src, wd[:, from_], preferred_element_type=F32).astype(BF16)
            part[d, :, :, :, cols] = y.reshape(2, 2, rows, piece)

        each(0, half // piece, down)
        sum_c(d).start()
        pl.when(d >= 1)(lambda: stage_x(d - 1))
        pl.when(d >= 3)(lambda: stage_z(d - 3))

    each(0, 2 * ns, feed)
    stage_x(2 * ns - 1)
    stage_z(2 * ns - 3)
    for d in (6, 7):
        cols = slice((d - 6) * half, (d - 5) * half)
        sum_x(d).wait_recv()
        sum_z(d - 4).wait_recv()
        sum_z(d - 2).wait_recv()
        resid[:, cols] += (
            keep[d] + xrecv[d].astype(F32) + zrecv[d - 4].astype(F32) + zrecv[d - 2].astype(F32)
        )
    out_ref[...] = resid[...].astype(BF16)

    @pl.when(s + 1 < ns)
    def _():
        def sent(i):
            for copy in kv_out(i, kbuf.at[0], vbuf.at[0]):
                copy.wait_send()

        each(0, s + 1, sent)

    row_far(far).wait_send()
    row_z(s, near).wait_send()
    row_z(far, near).wait_send()
    for mat in range(3):
        others(lambda i, mat=mat: sized(i, lambda skip: weight_out(mat, i, skip).wait_send()))
        others(lambda i, mat=mat: sized(s, lambda skip: weight_pass(mat, i, g, skip).wait_send()))
    for j in range(1, nt):
        head_copy(j).wait_send()

    def spread_done(i):
        row_x(i, t).wait_send()
        row_c(0, i, t).wait_send()
        row_c(1, i, tx).wait_send()

    each(0, ns, spread_done)

    def sums_done(d):
        sum_c(d).wait_send()
        sum_x(d).wait_send()

    each(0, 2 * ns, sums_done)
    each(0, 2 * ns - 2, lambda d: sum_z(d).wait_send())


def fused(ns, nt, chunk, resid_in, queries, keys, values, cum_gate, w_out, norm_gain, w_gate, w_up, w_down):
    rows, width = resid_in.shape
    tok, att_w = queries.shape
    depth, units = w_gate.shape
    nheads = att_w // HEAD_DIM
    vm = pl.BlockSpec(memory_space=pltpu.VMEM)
    hbm = pl.BlockSpec(memory_space=pltpu.HBM)
    dma = pltpu.SemaphoreType.DMA
    return pl.pallas_call(
        functools.partial(layer_kernel, (ns, nt, chunk)),
        out_shape=jax.ShapeDtypeStruct((rows, width), BF16),
        in_specs=[vm] * 6 + [hbm] * 4,
        out_specs=vm,
        scratch_shapes=[
            pltpu.VMEM((ns - 1, tok, att_w), BF16),
            pltpu.VMEM((ns - 1, tok, att_w), BF16),
            pltpu.VMEM((nheads, tok, 1), F32),
            pltpu.VMEM((nheads, tok, 1), F32),
            pltpu.VMEM((nheads, tok, HEAD_DIM), F32),
            pltpu.VMEM((tok, att_w), BF16),
            pltpu.VMEM((nt - 1, rows, att_w), BF16),
            pltpu.VMEM(w_out.shape, BF16),
            pltpu.VMEM((rows, width), F32),
            pltpu.VMEM((ns, nt, rows, width), BF16),
            pltpu.VMEM((width, chunk), BF16),
            pltpu.VMEM((width, chunk), BF16),
            pltpu.VMEM((chunk, width), BF16),
            pltpu.VMEM((ns, tok, chunk), BF16),
            pltpu.VMEM((2 * ns, 2, 2, rows, width // 2), BF16),
            pltpu.VMEM((2 * ns, 2, rows, width // 2), BF16),
            pltpu.VMEM((2 * ns, rows, width // 2), BF16),
            pltpu.VMEM((2 * ns, rows, width // 2), F32),
            pltpu.VMEM((2 * ns, rows, width // 2), BF16),
            pltpu.VMEM((2 * ns, rows, width // 2), BF16),
            pltpu.VMEM((2 * ns, rows, width // 2), BF16),
            dma((4,)),
            dma((2, ns)), dma((2, ns)),
            dma((3, ns)), dma((3, ns)),
            dma((3, ns)), dma((3, ns)),
            dma((nt - 1,)), dma((nt - 1,)),
            dma((2, ns)), dma((ns,)),
            dma((ns,)), dma((ns,)),
            dma((2, ns)), dma((2, ns)),
            dma((2 * ns,)), dma((2 * ns,)),
            dma((2 * ns,)), dma((2 * ns,)),
            dma((2 * ns,)), dma((2 * ns,)),
            pltpu.SemaphoreType.REGULAR,
        ],
        compiler_params=pltpu.CompilerParams(
            collective_id=0, has_side_effects=True, vmem_limit_bytes=60 * 2**20
        ),
        name="layer",
    )(
        resid_in, queries, keys, values, cum_gate.T, norm_gain[None, :], w_out, w_gate,
        w_up, w_down,
    )


def pick(mesh):
    ng, ns, nt = (mesh.shape[a] for a in ("grp", "sp", "tp"))

    def step(*args):
        resid_in, queries, cum_gate, w_gate = args[0], args[1], args[4], args[7]
        rows, width = resid_in.shape
        depth, units = w_gate.shape
        chunk = -(-units // (128 * ns)) * 128
        need = 2 * ns * nt * rows * width * 4 + 6 * width * chunk + 2 * args[5].size
        fits = (
            ng == 2 and nt == 4 and ns == 4 and units % 128 == 0 and (ns - 1) * chunk < units
            and depth % 256 == 0 and width % 256 == 0 and (chunk - ns * chunk + units) % 32 == 0 and width == ns * depth and rows % 16 == 0
            and queries.shape[0] == rows * nt and queries.shape[0] % 128 == 0
            and cum_gate.shape[0] == ns * nt * rows and queries.shape[1] % 128 == 0
            and need < 40 * 2**20
        )
        if fits:
            return fused(ns, nt, chunk, *args)
        return on_device(*args)

    return step


def solution(mesh):
    return jax.shard_map(
        pick(mesh),
        mesh=mesh,
        in_specs=(
            P(("grp", "sp", "tp"), None),
            P(("grp", "sp"), "tp"),
            P(("grp", "sp"), "tp"),
            P(("grp", "sp"), "tp"),
            P("grp", "tp"),
            P(),
            P(),
            P("sp", "tp"),
            P("sp", "tp"),
            P("tp", "sp"),
        ),
        out_specs=P(("grp", "sp", "tp"), None),
        check_vma=False,
    )
```

```python
import functools
import math

import jax
import jax.numpy as jnp
from jax import lax
from jax.experimental import pallas as pl
from jax.experimental.pallas import tpu as pltpu
from jax.sharding import PartitionSpec as P

HEAD_DIM = 64


def on_device(resid_in, queries, keys, values, cum_gate, w_out, norm_gain, w_gate, w_up, w_down):
    tok_rows = queries.shape[0]
    local_heads = queries.shape[1] // HEAD_DIM
    scale = HEAD_DIM ** (-0.5)
    offset = lax.axis_index("sp") * tok_rows
    query_heads = queries.reshape(tok_rows, local_heads, HEAD_DIM)
    own_gate = lax.dynamic_slice_in_dim(cum_gate, offset, tok_rows, 0).T
    query_pos = offset + jnp.arange(tok_rows, dtype=jnp.int32)
    last_pos = offset + tok_rows - 1
    initial = (
        jnp.full((local_heads, tok_rows), -1e30, jnp.float32),
        jnp.zeros((local_heads, tok_rows), jnp.float32),
        jnp.zeros((tok_rows, local_heads, HEAD_DIM), jnp.float32),
    )
    pair = lax.all_gather(jnp.stack([keys, values]), "sp", axis=1, tiled=True)
    key_piece, value_piece = pair[0], pair[1]
    length = key_piece.shape[0]
    span = math.gcd(length, 512)

    def block(index, state):
        begin = index * span

        def work(inner):
            maxima, totals, summed = inner
            key_block = lax.dynamic_slice_in_dim(key_piece, index * span, span, 0).reshape(
                span, local_heads, HEAD_DIM
            )
            value_block_rows = lax.dynamic_slice_in_dim(value_piece, index * span, span, 0).reshape(
                span, local_heads, HEAD_DIM
            )
            key_gate = lax.dynamic_slice_in_dim(cum_gate, begin, span, 0).T
            scores = (
                jnp.einsum(
                    "qhd,khd->hqk", query_heads, key_block, preferred_element_type=jnp.float32
                )
                * scale
            )
            scores = scores + own_gate[:, :, None] - key_gate[:, None, :]
            key_pos = begin + jnp.arange(span, dtype=jnp.int32)
            mask = (key_pos[None, :] <= query_pos[:, None])[None]
            scores = jnp.where(mask, scores, -1e30)
            new_max = jnp.maximum(maxima, jnp.max(scores, axis=-1))
            weights = jnp.where(mask, jnp.exp(scores - new_max[:, :, None]), 0.0)
            rescale = jnp.exp(maxima - new_max)
            totals = totals * rescale + jnp.sum(weights, axis=-1)
            product = jnp.einsum(
                "hqk,khd->qhd",
                weights.astype(jnp.bfloat16),
                value_block_rows,
                preferred_element_type=jnp.float32,
            )
            summed = summed * rescale.T[:, :, None] + product
            return (new_max, totals, summed)

        return lax.cond(begin <= last_pos, work, lambda inner: inner, state)

    maxima, totals, summed = lax.fori_loop(0, length // span, block, initial)
    attended = (
        (summed / totals.T[:, :, None])
        .reshape(tok_rows, local_heads * HEAD_DIM)
        .astype(jnp.bfloat16)
    )
    head_rows = lax.all_to_all(attended, "tp", split_axis=0, concat_axis=1, tiled=True)
    mixed = jnp.dot(head_rows, w_out, preferred_element_type=jnp.float32)
    resid = resid_in.astype(jnp.float32) + mixed
    normed = resid * lax.rsqrt(jnp.mean(resid * resid, axis=-1, keepdims=True) + 1e-06)
    normed = (normed * norm_gain).astype(jnp.bfloat16)
    all_rows = lax.all_gather(normed, ("sp", "tp"), axis=0, tiled=True)
    full_gate, full_up, full_down = (
        lax.all_to_all(w_gate, "sp", split_axis=1, concat_axis=0, tiled=True),
        lax.all_to_all(w_up, "sp", split_axis=1, concat_axis=0, tiled=True),
        lax.all_to_all(w_down, "sp", split_axis=0, concat_axis=1, tiled=True),
    )
    gate = jnp.dot(all_rows, full_gate, preferred_element_type=jnp.float32)
    up = jnp.dot(all_rows, full_up, preferred_element_type=jnp.float32)
    hidden = (jax.nn.silu(gate) * up).astype(jnp.bfloat16)
    terms = jnp.dot(hidden, full_down, preferred_element_type=jnp.float32)
    back = lax.psum_scatter(
        terms.astype(jnp.bfloat16), ("sp", "tp"), scatter_dimension=0, tiled=True
    ).astype(jnp.float32)
    return (resid + back).astype(jnp.bfloat16)


MESH = pl.DeviceIdType.MESH
F32 = jnp.float32
BF16 = jnp.bfloat16


def layer_kernel(
    dims, resid_ref, q_ref, k_ref, v_ref, gate_t_ref, gain_ref, w_out_ref, w_gate_ref,
    w_up_ref, w_down_ref, out_ref, kbuf, vbuf, top, tot, acc, att, heads, w_out, resid, nall, wg,
    wu, wd, hidden, part, crecv, csend, keep, xrecv, zsend, zrecv, loc_sem, kv_send, kv_recv, wz_send,
    wz_recv, wy_send, wy_recv, h_send, h_recv, az_send, az_recv, ax_send, ax_recv, ac_send,
    ac_recv, rc_send, rc_recv, rx_send, rx_recv, rz_send, rz_recv, go,
):
    ns, nt, chunk = dims
    g, s, t = lax.axis_index("grp"), lax.axis_index("sp"), lax.axis_index("tp")
    rows, width = resid_ref.shape
    tok, att_w = q_ref.shape
    depth, units = w_gate_ref.shape
    nheads = att_w // HEAD_DIM
    half_depth = depth // 2
    dup = ns * chunk - units
    x, c = t // 2, t % 2
    tx = (t + 2) % 4
    tc = t + 1 - 2 * c
    scale = HEAD_DIM ** (-0.5)

    def start_of(i):
        return pl.multiple_of(jnp.minimum(i * chunk, units - chunk), 128)

    def remote(src, dst, send, recv, **where):
        return pltpu.make_async_remote_copy(
            src_ref=src, dst_ref=dst, send_sem=send, recv_sem=recv, device_id=where,
            device_id_type=MESH,
        )

    def xor(a, b):
        hi, lo, bh, bl = a // 2, a % 2, b // 2, b % 2
        return 2 * (hi + bh - 2 * hi * bh) + lo + bl - 2 * lo * bl

    def landing(mat, src, half, skip):
        if mat < 2:
            return (wg, wu)[mat].at[
                pl.ds(pl.multiple_of(src * depth + half * half_depth, half_depth), half_depth),
                pl.ds(skip, chunk - skip),
            ]
        size = (chunk - skip) // 2
        return wd.at[
            pl.ds(pl.multiple_of(skip + half * size, math.gcd(128, size)), size),
            pl.ds(pl.multiple_of(src * depth, depth), depth),
        ]

    def weight_out(mat, dst, skip):
        if mat < 2:
            src = (w_gate_ref, w_up_ref)[mat].at[
                pl.ds(pl.multiple_of(g * half_depth, half_depth), half_depth),
                pl.ds(pl.multiple_of(start_of(dst) + skip, 128), chunk - skip),
            ]
        else:
            size = (chunk - skip) // 2
            src = w_down_ref.at[
                pl.ds(pl.multiple_of(start_of(dst) + skip + g * size, math.gcd(128, size)), size)
            ]
        return remote(
            src, landing(mat, s, g, skip), wz_send.at[mat, dst], wz_recv.at[mat, s], sp=dst
        )

    def weight_in(mat, src, skip):
        block = landing(mat, src, g, skip)
        return remote(block, block, wz_send.at[mat, src], wz_recv.at[mat, src], sp=src)

    def weight_pass(mat, src, half, skip):
        block = landing(mat, src, half, skip)
        return remote(block, block, wy_send.at[mat, src], wy_recv.at[mat, src], grp=1 - g)

    def sized(dst, body):
        pl.when(dst < ns - 1)(lambda: body(0))
        pl.when(dst == ns - 1)(lambda: body(dup))

    def each(low, high, body):
        lax.fori_loop(low, high, lambda i, z: (body(i), z)[1], 0)

    def others(body):
        each(0, s, body)
        each(s + 1, ns, body)

    barrier = pltpu.get_barrier_semaphore()
    others(lambda i: pl.semaphore_signal(barrier, inc=1, device_id={"sp": i}, device_id_type=MESH))
    pl.semaphore_signal(barrier, inc=1, device_id={"grp": 1 - g}, device_id_type=MESH)
    for j in range(1, nt):
        pl.semaphore_signal(barrier, inc=1, device_id={"tp": (t + j) % nt}, device_id_type=MESH)
    pl.semaphore_wait(barrier, ns + nt - 1)

    def kv_out(i, kk, vv):
        return (
            remote(kk, kbuf.at[i], kv_send.at[0, i], kv_recv.at[0, i], sp=s + 1),
            remote(vv, vbuf.at[i], kv_send.at[1, i], kv_recv.at[1, i], sp=s + 1),
        )

    def kv_in(i):
        return (
            remote(kbuf.at[i], kbuf.at[i], kv_send.at[0, i], kv_recv.at[0, i], sp=s - 1),
            remote(vbuf.at[i], vbuf.at[i], kv_send.at[1, i], kv_recv.at[1, i], sp=s - 1),
        )

    @pl.when(s + 1 < ns)
    def _():
        for copy in kv_out(0, k_ref, v_ref):
            copy.start()

    def locals_():
        own = pl.ds(pl.multiple_of(s * depth, depth), depth)
        return (
            pltpu.make_async_copy(w_out_ref, w_out, loc_sem.at[0]),
            pltpu.make_async_copy(w_gate_ref.at[:, pl.ds(start_of(s), chunk)], wg.at[own], loc_sem.at[1]),
            pltpu.make_async_copy(w_up_ref.at[:, pl.ds(start_of(s), chunk)], wu.at[own], loc_sem.at[2]),
            pltpu.make_async_copy(w_down_ref.at[pl.ds(start_of(s), chunk)], wd.at[:, own], loc_sem.at[3]),
        )

    for copy in locals_():
        copy.start()
    def send_weight(mat, dst):
        sized(dst, lambda skip: weight_out(mat, dst, skip).start())

    for mat in range(2):
        each(0, s, lambda i, mat=mat: send_weight(mat, s - 1 - i))

    if dup:

        @pl.when(s == ns - 1)
        def _():
            for mat in range(2):
                def clear(i, mat=mat):
                    band = pl.ds(pl.multiple_of((i + (i >= s)) * depth, depth), depth)
                    (wg, wu)[mat][band, :dup] = jnp.zeros((depth, dup), BF16)

                each(0, ns - 1, clear)
            wd[:dup, : (ns - 1) * depth] = jnp.zeros((dup, (ns - 1) * depth), BF16)

    gate_own = gate_t_ref[:, pl.ds(pl.multiple_of(s * tok, tok), tok)].T

    def attend(src, kk, vv, first):
        for h in range(nheads):
            lanes = slice(h * HEAD_DIM, (h + 1) * HEAD_DIM)
            scores = lax.dot_general(
                q_ref[:, lanes], kk[:, lanes], (((1,), (1,)), ((), ())), preferred_element_type=F32
            )
            key_gate = gate_t_ref[h : h + 1, pl.ds(pl.multiple_of(src * tok, tok), tok)]
            scores = scores * scale + gate_own[:, h : h + 1] - key_gate
            if first:
                row = lax.broadcasted_iota(jnp.int32, (tok, tok), 0)
                col = lax.broadcasted_iota(jnp.int32, (tok, tok), 1)
                scores = jnp.where(col <= row, scores, -1e30)
                new = jnp.max(scores, axis=-1, keepdims=True)
                w = jnp.where(col <= row, jnp.exp(scores - new), 0.0)
                tot[h] = jnp.sum(w, axis=-1, keepdims=True)
                acc[h] = jnp.dot(w.astype(BF16), vv[:, lanes], preferred_element_type=F32)
            else:
                old = top[h]
                new = jnp.maximum(old, jnp.max(scores, axis=-1, keepdims=True))
                w = jnp.exp(scores - new)
                shrink = jnp.exp(old - new)
                tot[h] = tot[h] * shrink + jnp.sum(w, axis=-1, keepdims=True)
                acc[h] = acc[h] * shrink + jnp.dot(
                    w.astype(BF16), vv[:, lanes], preferred_element_type=F32
                )
            top[h] = new

    attend(s, k_ref, v_ref, True)

    def earlier(i):
        for copy in kv_in(i - 1):
            copy.wait_recv()

        @pl.when(s + 1 < ns)
        def _():
            for copy in kv_out(i, kbuf.at[i - 1], vbuf.at[i - 1]):
                copy.start()

        @pl.when((i == s) & (s == ns - 2))
        def _():
            each(
                0, s,
                lambda j: pl.semaphore_signal(
                    go, inc=1, device_id={"sp": j}, device_id_type=MESH
                ),
            )

        attend(s - i, kbuf.at[i - 1], vbuf.at[i - 1], False)

    each(1, s + 1, earlier)

    for h in range(nheads):
        att[:, h * HEAD_DIM : (h + 1) * HEAD_DIM] = (acc[h] / tot[h]).astype(BF16)

    def head_copy(j):
        dst = (t + j) % nt
        return remote(
            att.at[pl.ds(pl.multiple_of(dst * rows, rows), rows)], heads.at[j - 1],
            h_send.at[j - 1], h_recv.at[j - 1], tp=dst,
        )

    for j in range(1, nt):
        head_copy(j).start()

    def pass_on(mat, src):
        def body(skip):
            weight_in(mat, src, skip).wait_recv()
            weight_pass(mat, src, g, skip).start()

        sized(s, body)

    copies = locals_()
    copies[0].wait()
    resid[...] = resid_ref[...].astype(F32) + jnp.dot(
        att[pl.ds(pl.multiple_of(t * rows, rows), rows), :],
        w_out[pl.ds(pl.multiple_of(t * att_w, att_w), att_w), :], preferred_element_type=F32,
    )

    def mix(j):
        head_copy(j).wait_recv()
        src = (t + nt - j) % nt
        resid[...] += jnp.dot(
            heads[j - 1], w_out[pl.ds(pl.multiple_of(src * att_w, att_w), att_w), :],
            preferred_element_type=F32,
        )

    each(1, nt, mix)
    full = resid[...]
    normed = full * lax.rsqrt(jnp.mean(full * full, axis=-1, keepdims=True) + 1e-06)
    nall[s, t] = (normed * gain_ref[...]).astype(BF16)

    def row_z(src, to):
        block = nall.at[src, t]
        return remote(block, block, az_send.at[0, src], az_recv.at[src], sp=to)

    def row_far(to):
        block = nall.at[s, t]
        return remote(block, block, az_send.at[1, s], az_recv.at[s], sp=to)

    def row_x(src, who):
        block = nall.at[src, who]
        return remote(block, block, ax_send.at[src], ax_recv.at[src], tp=tx)

    def row_c(kind, src, who):
        block = nall.at[src, who]
        return remote(block, block, ac_send.at[kind, src], ac_recv.at[kind, src], tp=tc)

    def spread(src):
        row_x(src, t).start()
        row_c(0, src, t).start()

    def relay(src):
        row_x(src, tx).wait_recv()
        row_c(1, src, tx).start()

    near, far, cross = xor(s, 1), xor(s, 2), xor(s, 3)
    pl.when(s < ns - 2)(lambda: pl.semaphore_wait(go, 1))
    row_far(far).start()
    row_z(s, near).start()
    for mat in range(2):
        each(s + 1, ns, lambda i, mat=mat: send_weight(mat, i))
    each(0, s, lambda i: send_weight(2, s - 1 - i))
    each(s + 1, ns, lambda i: send_weight(2, i))
    spread(s)

    def take_far():
        row_z(far, far).wait_recv()
        row_z(far, near).start()
        spread(far)

    def take(src):
        row_z(src, near).wait_recv()
        spread(src)

    for mat in range(2):
        each(s + 1, ns, lambda i, mat=mat: pass_on(mat, i))
    relay(s)
    pl.when(s >= 2)(take_far)
    for mat in range(2):
        each(0, s, lambda i, mat=mat: pass_on(mat, s - 1 - i))
    pl.when(s < 2)(take_far)
    take(near)
    relay(far)
    take(cross)
    each(s + 1, ns, lambda i: pass_on(2, i))
    each(0, s, lambda i: pass_on(2, s - 1 - i))
    relay(near)
    relay(cross)

    for copy in copies[1:]:
        copy.wait()

    def twin_in(mat):
        others(lambda i: sized(s, lambda skip: weight_pass(mat, i, 1 - g, skip).wait_recv()))

    twin_in(0)
    twin_in(1)
    fresh = lax.broadcasted_iota(jnp.int32, (tok, chunk), 1) + start_of(s) >= s * chunk
    half = width // 2
    piece = math.gcd(half, 512)

    def hide(src):
        row_c(0, src, tc).wait_recv()
        row_c(1, src, (tc + 2) % 4).wait_recv()
        a = nall[src].reshape(tok, width)
        gate = jnp.dot(a, wg[...], preferred_element_type=F32)
        up = jnp.dot(a, wu[...], preferred_element_type=F32)
        hidden[src] = jnp.where(fresh, gate / (1.0 + jnp.exp(-gate)) * up, 0.0).astype(BF16)

    each(0, ns, lambda k: hide(xor(s, k)))
    twin_in(2)

    def sum_c(d):
        return remote(part.at[d, :, 1 - c], crecv.at[d], rc_send.at[d], rc_recv.at[d], tp=tc)

    def sum_x(d):
        return remote(csend.at[d], xrecv.at[d], rx_send.at[d], rx_recv.at[d], tp=tx)

    def sum_z(d):
        return remote(zsend.at[d], zrecv.at[d], rz_send.at[d], rz_recv.at[d], sp=xor(s, 1 + d // 2 % 2))

    def stage_x(d):
        sum_c(d).wait_recv()
        csend[d] = (part[d, 1 - x, c].astype(F32) + crecv[d, 1 - x].astype(F32)).astype(BF16)
        sum_x(d).start()
        keep[d] = part[d, x, c].astype(F32) + crecv[d, x].astype(F32)

    def stage_z(d):
        sum_x(d).wait_recv()
        keep[d] = keep[d] + xrecv[d].astype(F32)

        @pl.when((d == 2) | (d == 3))
        def _():
            sum_z(d - 2).wait_recv()
            keep[d] = keep[d] + zrecv[d - 2].astype(F32)

        zsend[d] = keep[d].astype(BF16)
        sum_z(d).start()

    def feed(d):
        src = hidden[xor(s, 3 - d // 2)]

        def down(p):
            cols = pl.ds(pl.multiple_of(p * piece, piece), piece)
            from_ = pl.ds(pl.multiple_of(d % 2 * half + p * piece, piece), piece)
            y = jnp.dot(src, wd[:, from_], preferred_element_type=F32).astype(BF16)
            part[d, :, :, :, cols] = y.reshape(2, 2, rows, piece)

        each(0, half // piece, down)
        sum_c(d).start()
        pl.when(d >= 1)(lambda: stage_x(d - 1))
        pl.when(d >= 3)(lambda: stage_z(d - 3))

    each(0, 2 * ns, feed)
    stage_x(2 * ns - 1)
    stage_z(2 * ns - 3)
    for d in (6, 7):
        cols = slice((d - 6) * half, (d - 5) * half)
        sum_x(d).wait_recv()
        sum_z(d - 4).wait_recv()
        sum_z(d - 2).wait_recv()
        resid[:, cols] += (
            keep[d] + xrecv[d].astype(F32) + zrecv[d - 4].astype(F32) + zrecv[d - 2].astype(F32)
        )
    out_ref[...] = resid[...].astype(BF16)

    @pl.when(s + 1 < ns)
    def _():
        def sent(i):
            for copy in kv_out(i, kbuf.at[0], vbuf.at[0]):
                copy.wait_send()

        each(0, s + 1, sent)

    row_far(far).wait_send()
    row_z(s, near).wait_send()
    row_z(far, near).wait_send()
    for mat in range(3):
        others(lambda i, mat=mat: sized(i, lambda skip: weight_out(mat, i, skip).wait_send()))
        others(lambda i, mat=mat: sized(s, lambda skip: weight_pass(mat, i, g, skip).wait_send()))
    for j in range(1, nt):
        head_copy(j).wait_send()

    def spread_done(i):
        row_x(i, t).wait_send()
        row_c(0, i, t).wait_send()
        row_c(1, i, tx).wait_send()

    each(0, ns, spread_done)

    def sums_done(d):
        sum_c(d).wait_send()
        sum_x(d).wait_send()

    each(0, 2 * ns, sums_done)
    each(0, 2 * ns - 2, lambda d: sum_z(d).wait_send())


def fused(ns, nt, chunk, resid_in, queries, keys, values, cum_gate, w_out, norm_gain, w_gate, w_up, w_down):
    rows, width = resid_in.shape
    tok, att_w = queries.shape
    depth, units = w_gate.shape
    nheads = att_w // HEAD_DIM
    vm = pl.BlockSpec(memory_space=pltpu.VMEM)
    hbm = pl.BlockSpec(memory_space=pltpu.HBM)
    dma = pltpu.SemaphoreType.DMA
    return pl.pallas_call(
        functools.partial(layer_kernel, (ns, nt, chunk)),
        out_shape=jax.ShapeDtypeStruct((rows, width), BF16),
        in_specs=[vm] * 6 + [hbm] * 4,
        out_specs=vm,
        scratch_shapes=[
            pltpu.VMEM((ns - 1, tok, att_w), BF16),
            pltpu.VMEM((ns - 1, tok, att_w), BF16),
            pltpu.VMEM((nheads, tok, 1), F32),
            pltpu.VMEM((nheads, tok, 1), F32),
            pltpu.VMEM((nheads, tok, HEAD_DIM), F32),
            pltpu.VMEM((tok, att_w), BF16),
            pltpu.VMEM((nt - 1, rows, att_w), BF16),
            pltpu.VMEM(w_out.shape, BF16),
            pltpu.VMEM((rows, width), F32),
            pltpu.VMEM((ns, nt, rows, width), BF16),
            pltpu.VMEM((width, chunk), BF16),
            pltpu.VMEM((width, chunk), BF16),
            pltpu.VMEM((chunk, width), BF16),
            pltpu.VMEM((ns, tok, chunk), BF16),
            pltpu.VMEM((2 * ns, 2, 2, rows, width // 2), BF16),
            pltpu.VMEM((2 * ns, 2, rows, width // 2), BF16),
            pltpu.VMEM((2 * ns, rows, width // 2), BF16),
            pltpu.VMEM((2 * ns, rows, width // 2), F32),
            pltpu.VMEM((2 * ns, rows, width // 2), BF16),
            pltpu.VMEM((2 * ns, rows, width // 2), BF16),
            pltpu.VMEM((2 * ns, rows, width // 2), BF16),
            dma((4,)),
            dma((2, ns)), dma((2, ns)),
            dma((3, ns)), dma((3, ns)),
            dma((3, ns)), dma((3, ns)),
            dma((nt - 1,)), dma((nt - 1,)),
            dma((2, ns)), dma((ns,)),
            dma((ns,)), dma((ns,)),
            dma((2, ns)), dma((2, ns)),
            dma((2 * ns,)), dma((2 * ns,)),
            dma((2 * ns,)), dma((2 * ns,)),
            dma((2 * ns,)), dma((2 * ns,)),
            pltpu.SemaphoreType.REGULAR,
        ],
        compiler_params=pltpu.CompilerParams(
            collective_id=0, has_side_effects=True, vmem_limit_bytes=60 * 2**20
        ),
        name="layer",
    )(
        resid_in, queries, keys, values, cum_gate.T, norm_gain[None, :], w_out, w_gate,
        w_up, w_down,
    )


def pick(mesh):
    ng, ns, nt = (mesh.shape[a] for a in ("grp", "sp", "tp"))

    def step(*args):
        resid_in, queries, cum_gate, w_gate = args[0], args[1], args[4], args[7]
        rows, width = resid_in.shape
        depth, units = w_gate.shape
        chunk = -(-units // (128 * ns)) * 128
        need = 2 * ns * nt * rows * width * 4 + 6 * width * chunk + 2 * args[5].size
        fits = (
            ng == 2 and nt == 4 and ns == 4 and units % 128 == 0 and (ns - 1) * chunk < units
            and depth % 256 == 0 and width % 256 == 0 and (chunk - ns * chunk + units) % 32 == 0 and width == ns * depth and rows % 16 == 0
            and queries.shape[0] == rows * nt and queries.shape[0] % 128 == 0
            and cum_gate.shape[0] == ns * nt * rows and queries.shape[1] % 128 == 0
            and need < 40 * 2**20
        )
        if fits:
            return fused(ns, nt, chunk, *args)
        return on_device(*args)

    return step


def solution(mesh):
    return jax.shard_map(
        pick(mesh),
        mesh=mesh,
        in_specs=(
            P(("grp", "sp", "tp"), None),
            P(("grp", "sp"), "tp"),
            P(("grp", "sp"), "tp"),
            P(("grp", "sp"), "tp"),
            P("grp", "tp"),
            P(),
            P(),
            P("sp", "tp"),
            P("sp", "tp"),
            P("tp", "sp"),
        ),
        out_specs=P(("grp", "sp", "tp"), None),
        check_vma=False,
    )
```

```python
import functools
import math

import jax
import jax.numpy as jnp
from jax import lax
from jax.experimental import pallas as pl
from jax.experimental.pallas import tpu as pltpu
from jax.sharding import PartitionSpec as P

HEAD_DIM = 64


def on_device(resid_in, queries, keys, values, cum_gate, w_out, norm_gain, w_gate, w_up, w_down):
    tok_rows = queries.shape[0]
    local_heads = queries.shape[1] // HEAD_DIM
    scale = HEAD_DIM ** (-0.5)
    offset = lax.axis_index("sp") * tok_rows
    query_heads = queries.reshape(tok_rows, local_heads, HEAD_DIM)
    own_gate = lax.dynamic_slice_in_dim(cum_gate, offset, tok_rows, 0).T
    query_pos = offset + jnp.arange(tok_rows, dtype=jnp.int32)
    last_pos = offset + tok_rows - 1
    initial = (
        jnp.full((local_heads, tok_rows), -1e30, jnp.float32),
        jnp.zeros((local_heads, tok_rows), jnp.float32),
        jnp.zeros((tok_rows, local_heads, HEAD_DIM), jnp.float32),
    )
    pair = lax.all_gather(jnp.stack([keys, values]), "sp", axis=1, tiled=True)
    key_piece, value_piece = pair[0], pair[1]
    length = key_piece.shape[0]
    span = math.gcd(length, 512)

    def block(index, state):
        begin = index * span

        def work(inner):
            maxima, totals, summed = inner
            key_block = lax.dynamic_slice_in_dim(key_piece, index * span, span, 0).reshape(
                span, local_heads, HEAD_DIM
            )
            value_block_rows = lax.dynamic_slice_in_dim(value_piece, index * span, span, 0).reshape(
                span, local_heads, HEAD_DIM
            )
            key_gate = lax.dynamic_slice_in_dim(cum_gate, begin, span, 0).T
            scores = (
                jnp.einsum(
                    "qhd,khd->hqk", query_heads, key_block, preferred_element_type=jnp.float32
                )
                * scale
            )
            scores = scores + own_gate[:, :, None] - key_gate[:, None, :]
            key_pos = begin + jnp.arange(span, dtype=jnp.int32)
            mask = (key_pos[None, :] <= query_pos[:, None])[None]
            scores = jnp.where(mask, scores, -1e30)
            new_max = jnp.maximum(maxima, jnp.max(scores, axis=-1))
            weights = jnp.where(mask, jnp.exp(scores - new_max[:, :, None]), 0.0)
            rescale = jnp.exp(maxima - new_max)
            totals = totals * rescale + jnp.sum(weights, axis=-1)
            product = jnp.einsum(
                "hqk,khd->qhd",
                weights.astype(jnp.bfloat16),
                value_block_rows,
                preferred_element_type=jnp.float32,
            )
            summed = summed * rescale.T[:, :, None] + product
            return (new_max, totals, summed)

        return lax.cond(begin <= last_pos, work, lambda inner: inner, state)

    maxima, totals, summed = lax.fori_loop(0, length // span, block, initial)
    attended = (
        (summed / totals.T[:, :, None])
        .reshape(tok_rows, local_heads * HEAD_DIM)
        .astype(jnp.bfloat16)
    )
    head_rows = lax.all_to_all(attended, "tp", split_axis=0, concat_axis=1, tiled=True)
    mixed = jnp.dot(head_rows, w_out, preferred_element_type=jnp.float32)
    resid = resid_in.astype(jnp.float32) + mixed
    normed = resid * lax.rsqrt(jnp.mean(resid * resid, axis=-1, keepdims=True) + 1e-06)
    normed = (normed * norm_gain).astype(jnp.bfloat16)
    all_rows = lax.all_gather(normed, ("sp", "tp"), axis=0, tiled=True)
    full_gate, full_up, full_down = (
        lax.all_to_all(w_gate, "sp", split_axis=1, concat_axis=0, tiled=True),
        lax.all_to_all(w_up, "sp", split_axis=1, concat_axis=0, tiled=True),
        lax.all_to_all(w_down, "sp", split_axis=0, concat_axis=1, tiled=True),
    )
    gate = jnp.dot(all_rows, full_gate, preferred_element_type=jnp.float32)
    up = jnp.dot(all_rows, full_up, preferred_element_type=jnp.float32)
    hidden = (jax.nn.silu(gate) * up).astype(jnp.bfloat16)
    terms = jnp.dot(hidden, full_down, preferred_element_type=jnp.float32)
    back = lax.psum_scatter(
        terms.astype(jnp.bfloat16), ("sp", "tp"), scatter_dimension=0, tiled=True
    ).astype(jnp.float32)
    return (resid + back).astype(jnp.bfloat16)


MESH = pl.DeviceIdType.MESH
F32 = jnp.float32
BF16 = jnp.bfloat16


def layer_kernel(
    dims, resid_ref, q_ref, k_ref, v_ref, gate_t_ref, gain_ref, w_out_ref, w_gate_ref,
    w_up_ref, w_down_ref, out_ref, kbuf, vbuf, top, tot, acc, att, heads, w_out, resid, nall, wg,
    wu, wd, hidden, part, crecv, csend, keep, xrecv, zsend, zrecv, loc_sem, kv_send, kv_recv, wz_send,
    wz_recv, wy_send, wy_recv, h_send, h_recv, az_send, az_recv, ax_send, ax_recv, ac_send,
    ac_recv, rc_send, rc_recv, rx_send, rx_recv, rz_send, rz_recv, go,
):
    ns, nt, chunk = dims
    g, s, t = lax.axis_index("grp"), lax.axis_index("sp"), lax.axis_index("tp")
    rows, width = resid_ref.shape
    tok, att_w = q_ref.shape
    depth, units = w_gate_ref.shape
    nheads = att_w // HEAD_DIM
    half_depth = depth // 2
    dup = ns * chunk - units
    x, c = t // 2, t % 2
    tx = (t + 2) % 4
    tc = t + 1 - 2 * c
    scale = HEAD_DIM ** (-0.5)

    def start_of(i):
        return pl.multiple_of(jnp.minimum(i * chunk, units - chunk), 128)

    def remote(src, dst, send, recv, **where):
        return pltpu.make_async_remote_copy(
            src_ref=src, dst_ref=dst, send_sem=send, recv_sem=recv, device_id=where,
            device_id_type=MESH,
        )

    def xor(a, b):
        hi, lo, bh, bl = a // 2, a % 2, b // 2, b % 2
        return 2 * (hi + bh - 2 * hi * bh) + lo + bl - 2 * lo * bl

    def landing(mat, src, half, skip):
        if mat < 2:
            return (wg, wu)[mat].at[
                pl.ds(pl.multiple_of(src * depth + half * half_depth, half_depth), half_depth),
                pl.ds(skip, chunk - skip),
            ]
        size = (chunk - skip) // 2
        return wd.at[
            pl.ds(pl.multiple_of(skip + half * size, math.gcd(128, size)), size),
            pl.ds(pl.multiple_of(src * depth, depth), depth),
        ]

    def weight_out(mat, dst, skip):
        if mat < 2:
            src = (w_gate_ref, w_up_ref)[mat].at[
                pl.ds(pl.multiple_of(g * half_depth, half_depth), half_depth),
                pl.ds(pl.multiple_of(start_of(dst) + skip, 128), chunk - skip),
            ]
        else:
            size = (chunk - skip) // 2
            src = w_down_ref.at[
                pl.ds(pl.multiple_of(start_of(dst) + skip + g * size, math.gcd(128, size)), size)
            ]
        return remote(
            src, landing(mat, s, g, skip), wz_send.at[mat, dst], wz_recv.at[mat, s], sp=dst
        )

    def weight_in(mat, src, skip):
        block = landing(mat, src, g, skip)
        return remote(block, block, wz_send.at[mat, src], wz_recv.at[mat, src], sp=src)

    def weight_pass(mat, src, half, skip):
        block = landing(mat, src, half, skip)
        return remote(block, block, wy_send.at[mat, src], wy_recv.at[mat, src], grp=1 - g)

    def sized(dst, body):
        pl.when(dst < ns - 1)(lambda: body(0))
        pl.when(dst == ns - 1)(lambda: body(dup))

    def each(low, high, body):
        lax.fori_loop(low, high, lambda i, z: (body(i), z)[1], 0)

    def others(body):
        each(0, s, body)
        each(s + 1, ns, body)

    barrier = pltpu.get_barrier_semaphore()
    others(lambda i: pl.semaphore_signal(barrier, inc=1, device_id={"sp": i}, device_id_type=MESH))
    pl.semaphore_signal(barrier, inc=1, device_id={"grp": 1 - g}, device_id_type=MESH)
    for j in range(1, nt):
        pl.semaphore_signal(barrier, inc=1, device_id={"tp": (t + j) % nt}, device_id_type=MESH)
    pl.semaphore_wait(barrier, ns + nt - 1)

    def kv_out(i, kk, vv):
        return (
            remote(kk, kbuf.at[i], kv_send.at[0, i], kv_recv.at[0, i], sp=s + 1),
            remote(vv, vbuf.at[i], kv_send.at[1, i], kv_recv.at[1, i], sp=s + 1),
        )

    def kv_in(i):
        return (
            remote(kbuf.at[i], kbuf.at[i], kv_send.at[0, i], kv_recv.at[0, i], sp=s - 1),
            remote(vbuf.at[i], vbuf.at[i], kv_send.at[1, i], kv_recv.at[1, i], sp=s - 1),
        )

    @pl.when(s + 1 < ns)
    def _():
        for copy in kv_out(0, k_ref, v_ref):
            copy.start()

    def locals_():
        own = pl.ds(pl.multiple_of(s * depth, depth), depth)
        return (
            pltpu.make_async_copy(w_out_ref, w_out, loc_sem.at[0]),
            pltpu.make_async_copy(w_gate_ref.at[:, pl.ds(start_of(s), chunk)], wg.at[own], loc_sem.at[1]),
            pltpu.make_async_copy(w_up_ref.at[:, pl.ds(start_of(s), chunk)], wu.at[own], loc_sem.at[2]),
            pltpu.make_async_copy(w_down_ref.at[pl.ds(start_of(s), chunk)], wd.at[:, own], loc_sem.at[3]),
        )

    for copy in locals_():
        copy.start()
    def send_weight(mat, dst):
        sized(dst, lambda skip: weight_out(mat, dst, skip).start())

    for mat in range(2):
        each(0, s, lambda i, mat=mat: send_weight(mat, s - 1 - i))

    if dup:

        @pl.when(s == ns - 1)
        def _():
            for mat in range(2):
                def clear(i, mat=mat):
                    band = pl.ds(pl.multiple_of((i + (i >= s)) * depth, depth), depth)
                    (wg, wu)[mat][band, :dup] = jnp.zeros((depth, dup), BF16)

                each(0, ns - 1, clear)
            wd[:dup, : (ns - 1) * depth] = jnp.zeros((dup, (ns - 1) * depth), BF16)

    gate_own = gate_t_ref[:, pl.ds(pl.multiple_of(s * tok, tok), tok)].T

    def attend(src, kk, vv, first):
        for h in range(nheads):
            lanes = slice(h * HEAD_DIM, (h + 1) * HEAD_DIM)
            scores = lax.dot_general(
                q_ref[:, lanes], kk[:, lanes], (((1,), (1,)), ((), ())), preferred_element_type=F32
            )
            key_gate = gate_t_ref[h : h + 1, pl.ds(pl.multiple_of(src * tok, tok), tok)]
            scores = scores * scale + gate_own[:, h : h + 1] - key_gate
            if first:
                row = lax.broadcasted_iota(jnp.int32, (tok, tok), 0)
                col = lax.broadcasted_iota(jnp.int32, (tok, tok), 1)
                scores = jnp.where(col <= row, scores, -1e30)
                new = jnp.max(scores, axis=-1, keepdims=True)
                w = jnp.where(col <= row, jnp.exp(scores - new), 0.0)
                tot[h] = jnp.sum(w, axis=-1, keepdims=True)
                acc[h] = jnp.dot(w.astype(BF16), vv[:, lanes], preferred_element_type=F32)
            else:
                old = top[h]
                new = jnp.maximum(old, jnp.max(scores, axis=-1, keepdims=True))
                w = jnp.exp(scores - new)
                shrink = jnp.exp(old - new)
                tot[h] = tot[h] * shrink + jnp.sum(w, axis=-1, keepdims=True)
                acc[h] = acc[h] * shrink + jnp.dot(
                    w.astype(BF16), vv[:, lanes], preferred_element_type=F32
                )
            top[h] = new

    attend(s, k_ref, v_ref, True)

    def earlier(i):
        for copy in kv_in(i - 1):
            copy.wait_recv()

        @pl.when(s + 1 < ns)
        def _():
            for copy in kv_out(i, kbuf.at[i - 1], vbuf.at[i - 1]):
                copy.start()

        @pl.when((i == s) & (s == ns - 2))
        def _():
            each(
                0, s,
                lambda j: pl.semaphore_signal(
                    go, inc=1, device_id={"sp": j}, device_id_type=MESH
                ),
            )

        attend(s - i, kbuf.at[i - 1], vbuf.at[i - 1], False)

    each(1, s + 1, earlier)

    for h in range(nheads):
        att[:, h * HEAD_DIM : (h + 1) * HEAD_DIM] = (acc[h] / tot[h]).astype(BF16)

    def head_copy(j):
        dst = (t + j) % nt
        return remote(
            att.at[pl.ds(pl.multiple_of(dst * rows, rows), rows)], heads.at[j - 1],
            h_send.at[j - 1], h_recv.at[j - 1], tp=dst,
        )

    for j in range(1, nt):
        head_copy(j).start()

    def pass_on(mat, src):
        def body(skip):
            weight_in(mat, src, skip).wait_recv()
            weight_pass(mat, src, g, skip).start()

        sized(s, body)

    copies = locals_()
    copies[0].wait()
    resid[...] = resid_ref[...].astype(F32) + jnp.dot(
        att[pl.ds(pl.multiple_of(t * rows, rows), rows), :],
        w_out[pl.ds(pl.multiple_of(t * att_w, att_w), att_w), :], preferred_element_type=F32,
    )

    def mix(j):
        head_copy(j).wait_recv()
        src = (t + nt - j) % nt
        resid[...] += jnp.dot(
            heads[j - 1], w_out[pl.ds(pl.multiple_of(src * att_w, att_w), att_w), :],
            preferred_element_type=F32,
        )

    each(1, nt, mix)
    full = resid[...]
    normed = full * lax.rsqrt(jnp.mean(full * full, axis=-1, keepdims=True) + 1e-06)
    nall[s, t] = (normed * gain_ref[...]).astype(BF16)

    def row_z(src, to):
        block = nall.at[src, t]
        return remote(block, block, az_send.at[0, src], az_recv.at[src], sp=to)

    def row_far(to):
        block = nall.at[s, t]
        return remote(block, block, az_send.at[1, s], az_recv.at[s], sp=to)

    def row_x(src, who):
        block = nall.at[src, who]
        return remote(block, block, ax_send.at[src], ax_recv.at[src], tp=tx)

    def row_c(kind, src, who):
        block = nall.at[src, who]
        return remote(block, block, ac_send.at[kind, src], ac_recv.at[kind, src], tp=tc)

    def spread(src):
        row_x(src, t).start()
        row_c(0, src, t).start()

    def relay(src):
        row_x(src, tx).wait_recv()
        row_c(1, src, tx).start()

    near, far, cross = xor(s, 1), xor(s, 2), xor(s, 3)
    pl.when(s < ns - 2)(lambda: pl.semaphore_wait(go, 1))
    row_far(far).start()
    row_z(s, near).start()
    for mat in range(2):
        each(s + 1, ns, lambda i, mat=mat: send_weight(mat, i))
    each(0, s, lambda i: send_weight(2, s - 1 - i))
    each(s + 1, ns, lambda i: send_weight(2, i))
    spread(s)

    def take_far():
        row_z(far, far).wait_recv()
        row_z(far, near).start()
        spread(far)

    def take(src):
        row_z(src, near).wait_recv()
        spread(src)

    for mat in range(2):
        each(s + 1, ns, lambda i, mat=mat: pass_on(mat, i))
    relay(s)
    pl.when(s >= 2)(take_far)
    for mat in range(2):
        each(0, s, lambda i, mat=mat: pass_on(mat, s - 1 - i))
    pl.when(s < 2)(take_far)
    take(near)
    take(cross)
    each(s + 1, ns, lambda i: pass_on(2, i))
    each(0, s, lambda i: pass_on(2, s - 1 - i))
    relay(far)
    relay(near)
    relay(cross)

    for copy in copies[1:]:
        copy.wait()

    def twin_in(mat):
        others(lambda i: sized(s, lambda skip: weight_pass(mat, i, 1 - g, skip).wait_recv()))

    twin_in(0)
    twin_in(1)
    fresh = lax.broadcasted_iota(jnp.int32, (tok, chunk), 1) + start_of(s) >= s * chunk
    half = width // 2
    piece = math.gcd(half, 512)

    def hide(src):
        row_c(0, src, tc).wait_recv()
        row_c(1, src, (tc + 2) % 4).wait_recv()
        a = nall[src].reshape(tok, width)
        gate = jnp.dot(a, wg[...], preferred_element_type=F32)
        up = jnp.dot(a, wu[...], preferred_element_type=F32)
        hidden[src] = jnp.where(fresh, gate / (1.0 + jnp.exp(-gate)) * up, 0.0).astype(BF16)

    each(0, ns, lambda k: hide(xor(s, k)))
    twin_in(2)

    def sum_c(d):
        return remote(part.at[d, :, 1 - c], crecv.at[d], rc_send.at[d], rc_recv.at[d], tp=tc)

    def sum_x(d):
        return remote(csend.at[d], xrecv.at[d], rx_send.at[d], rx_recv.at[d], tp=tx)

    def sum_z(d):
        return remote(zsend.at[d], zrecv.at[d], rz_send.at[d], rz_recv.at[d], sp=xor(s, 1 + d // 2 % 2))

    def stage_x(d):
        sum_c(d).wait_recv()
        csend[d] = (part[d, 1 - x, c].astype(F32) + crecv[d, 1 - x].astype(F32)).astype(BF16)
        sum_x(d).start()
        keep[d] = part[d, x, c].astype(F32) + crecv[d, x].astype(F32)

    def stage_z(d):
        sum_x(d).wait_recv()
        keep[d] = keep[d] + xrecv[d].astype(F32)

        @pl.when((d == 2) | (d == 3))
        def _():
            sum_z(d - 2).wait_recv()
            keep[d] = keep[d] + zrecv[d - 2].astype(F32)

        zsend[d] = keep[d].astype(BF16)
        sum_z(d).start()

    def feed(d):
        src = hidden[xor(s, 3 - d // 2)]

        def down(p):
            cols = pl.ds(pl.multiple_of(p * piece, piece), piece)
            from_ = pl.ds(pl.multiple_of(d % 2 * half + p * piece, piece), piece)
            y = jnp.dot(src, wd[:, from_], preferred_element_type=F32).astype(BF16)
            part[d, :, :, :, cols] = y.reshape(2, 2, rows, piece)

        each(0, half // piece, down)
        sum_c(d).start()
        pl.when(d >= 1)(lambda: stage_x(d - 1))
        pl.when(d >= 3)(lambda: stage_z(d - 3))

    each(0, 2 * ns, feed)
    stage_x(2 * ns - 1)
    stage_z(2 * ns - 3)
    for d in (6, 7):
        cols = slice((d - 6) * half, (d - 5) * half)
        sum_x(d).wait_recv()
        sum_z(d - 4).wait_recv()
        sum_z(d - 2).wait_recv()
        resid[:, cols] += (
            keep[d] + xrecv[d].astype(F32) + zrecv[d - 4].astype(F32) + zrecv[d - 2].astype(F32)
        )
    out_ref[...] = resid[...].astype(BF16)

    @pl.when(s + 1 < ns)
    def _():
        def sent(i):
            for copy in kv_out(i, kbuf.at[0], vbuf.at[0]):
                copy.wait_send()

        each(0, s + 1, sent)

    row_far(far).wait_send()
    row_z(s, near).wait_send()
    row_z(far, near).wait_send()
    for mat in range(3):
        others(lambda i, mat=mat: sized(i, lambda skip: weight_out(mat, i, skip).wait_send()))
        others(lambda i, mat=mat: sized(s, lambda skip: weight_pass(mat, i, g, skip).wait_send()))
    for j in range(1, nt):
        head_copy(j).wait_send()

    def spread_done(i):
        row_x(i, t).wait_send()
        row_c(0, i, t).wait_send()
        row_c(1, i, tx).wait_send()

    each(0, ns, spread_done)

    def sums_done(d):
        sum_c(d).wait_send()
        sum_x(d).wait_send()

    each(0, 2 * ns, sums_done)
    each(0, 2 * ns - 2, lambda d: sum_z(d).wait_send())


def fused(ns, nt, chunk, resid_in, queries, keys, values, cum_gate, w_out, norm_gain, w_gate, w_up, w_down):
    rows, width = resid_in.shape
    tok, att_w = queries.shape
    depth, units = w_gate.shape
    nheads = att_w // HEAD_DIM
    vm = pl.BlockSpec(memory_space=pltpu.VMEM)
    hbm = pl.BlockSpec(memory_space=pltpu.HBM)
    dma = pltpu.SemaphoreType.DMA
    return pl.pallas_call(
        functools.partial(layer_kernel, (ns, nt, chunk)),
        out_shape=jax.ShapeDtypeStruct((rows, width), BF16),
        in_specs=[vm] * 6 + [hbm] * 4,
        out_specs=vm,
        scratch_shapes=[
            pltpu.VMEM((ns - 1, tok, att_w), BF16),
            pltpu.VMEM((ns - 1, tok, att_w), BF16),
            pltpu.VMEM((nheads, tok, 1), F32),
            pltpu.VMEM((nheads, tok, 1), F32),
            pltpu.VMEM((nheads, tok, HEAD_DIM), F32),
            pltpu.VMEM((tok, att_w), BF16),
            pltpu.VMEM((nt - 1, rows, att_w), BF16),
            pltpu.VMEM(w_out.shape, BF16),
            pltpu.VMEM((rows, width), F32),
            pltpu.VMEM((ns, nt, rows, width), BF16),
            pltpu.VMEM((width, chunk), BF16),
            pltpu.VMEM((width, chunk), BF16),
            pltpu.VMEM((chunk, width), BF16),
            pltpu.VMEM((ns, tok, chunk), BF16),
            pltpu.VMEM((2 * ns, 2, 2, rows, width // 2), BF16),
            pltpu.VMEM((2 * ns, 2, rows, width // 2), BF16),
            pltpu.VMEM((2 * ns, rows, width // 2), BF16),
            pltpu.VMEM((2 * ns, rows, width // 2), F32),
            pltpu.VMEM((2 * ns, rows, width // 2), BF16),
            pltpu.VMEM((2 * ns, rows, width // 2), BF16),
            pltpu.VMEM((2 * ns, rows, width // 2), BF16),
            dma((4,)),
            dma((2, ns)), dma((2, ns)),
            dma((3, ns)), dma((3, ns)),
            dma((3, ns)), dma((3, ns)),
            dma((nt - 1,)), dma((nt - 1,)),
            dma((2, ns)), dma((ns,)),
            dma((ns,)), dma((ns,)),
            dma((2, ns)), dma((2, ns)),
            dma((2 * ns,)), dma((2 * ns,)),
            dma((2 * ns,)), dma((2 * ns,)),
            dma((2 * ns,)), dma((2 * ns,)),
            pltpu.SemaphoreType.REGULAR,
        ],
        compiler_params=pltpu.CompilerParams(
            collective_id=0, has_side_effects=True, vmem_limit_bytes=60 * 2**20
        ),
        name="layer",
    )(
        resid_in, queries, keys, values, cum_gate.T, norm_gain[None, :], w_out, w_gate,
        w_up, w_down,
    )


def pick(mesh):
    ng, ns, nt = (mesh.shape[a] for a in ("grp", "sp", "tp"))

    def step(*args):
        resid_in, queries, cum_gate, w_gate = args[0], args[1], args[4], args[7]
        rows, width = resid_in.shape
        depth, units = w_gate.shape
        chunk = -(-units // (128 * ns)) * 128
        need = 2 * ns * nt * rows * width * 4 + 6 * width * chunk + 2 * args[5].size
        fits = (
            ng == 2 and nt == 4 and ns == 4 and units % 128 == 0 and (ns - 1) * chunk < units
            and depth % 256 == 0 and width % 256 == 0 and (chunk - ns * chunk + units) % 32 == 0 and width == ns * depth and rows % 16 == 0
            and queries.shape[0] == rows * nt and queries.shape[0] % 128 == 0
            and cum_gate.shape[0] == ns * nt * rows and queries.shape[1] % 128 == 0
            and need < 40 * 2**20
        )
        if fits:
            return fused(ns, nt, chunk, *args)
        return on_device(*args)

    return step


def solution(mesh):
    return jax.shard_map(
        pick(mesh),
        mesh=mesh,
        in_specs=(
            P(("grp", "sp", "tp"), None),
            P(("grp", "sp"), "tp"),
            P(("grp", "sp"), "tp"),
            P(("grp", "sp"), "tp"),
            P("grp", "tp"),
            P(),
            P(),
            P("sp", "tp"),
            P("sp", "tp"),
            P("tp", "sp"),
        ),
        out_specs=P(("grp", "sp", "tp"), None),
        check_vma=False,
    )
```
